32 devices in a mesh: rep: 2 (over x), fs: 8 (over z, y), tp: 2 (over core).
Axes of the slice: x: 2, y: 2, z: 4, core: 2. Of those that a mesh axis runs over, the one named last changes fastest.
Arguments:
- x_later: bfloat16 [2048, 2048], P(('rep', 'fs')), may hold values from -6 to 6
- kept_input_rows: bfloat16 [2048, 2048], P(('rep', 'fs')), may hold values from -6 to 6
- cotangent: bfloat16 [2048, 2048], P(('rep', 'fs')), may hold values from -8 to 8
- norm_gain_vector: float32 [2048], replicated, may hold values from 0.1 to 1.9
- up_weight: bfloat16 [2048, 4096], P('fs', 'tp'), may hold values from -0.125 to 0.125
- down_weight: bfloat16 [4096, 2048], P('tp', 'fs'), may hold values from -0.09375 to 0.09375
- up_sum: float32 [2048, 4096], P('fs', 'tp'), may hold values from -6 to 6
- down_sum: float32 [4096, 2048], P('tp', 'fs'), may hold values from -6 to 6
Outputs:
- mixed: bfloat16 [2048, 2048], P(('rep', 'fs'))
- input_gradient_rows: bfloat16 [2048, 2048], P(('rep', 'fs'))
- up_total: float32 [2048, 4096], P('fs', 'tp')
- down_total: float32 [4096, 2048], P('tp', 'fs')
The draws below stay inside these ranges and needn't reach their ends.
All inputs are finite; a program needn't handle non-finite values.
Results may differ from the reference program's by a relative error of at most 0.018.
Values may be sent and summed in bfloat16 or wider, within the bound.
A program may use at most 128 MiB of HBM per device.

```python
import jax
import jax.numpy as jnp
from jax import lax

D = 2048
FF = 4096
TOKENS = 2048
N_TP = 2


def with_spikes(values, own_key, source, target, shards_of, factor):
    def block_of(dim):
        return (jnp.arange(values.shape[dim]) // (values.shape[dim] // shards_of)).reshape((-1,) + (1,) * (values.ndim - 1 - dim))

    one_side = jax.random.permutation(own_key, shards_of)[block_of(target)]
    far = (block_of(target) + shards_of // 2) % shards_of
    return jnp.where((block_of(source) == one_side) | (block_of(source) == far), factor * values, values)


def block_scale(stream_key, extent, cuts, least, top_value):
    gain, own = 1.0, jax.random.fold_in(stream_key, 6)
    for position, blocks in cuts:
        draws = jnp.exp(jax.random.uniform(jax.random.fold_in(own, position), (blocks,), jnp.float32, least / len(cuts), top_value / len(cuts)))
        gain = gain * jnp.repeat(draws, extent[position] // blocks).reshape([-1 if axis == position else 1 for axis in range(len(extent))])
    return gain


def bell_draw(key, shape, scale, most, cuts=(), kind=jnp.bfloat16):
    entries = scale * jax.random.normal(key, shape, jnp.float32)
    if cuts:
        entries = entries * block_scale(key, shape, cuts, -0.22, 0.18)
    return jnp.clip(entries, -most, most).astype(kind)


def gaussian_with(stream_key, dims, scale, limit, pieces, heavy, held_as=jnp.bfloat16):
    entries = scale * jax.random.normal(stream_key, dims, jnp.float32)
    if pieces:
        entries = entries * block_scale(stream_key, dims, pieces, -0.22, 0.18)
    return jnp.clip(with_spikes(entries, jax.random.fold_in(stream_key, 3), *heavy), -limit, limit).astype(held_as)


def setup_inputs(seed: int = 0) -> dict:
    key_list = jax.random.split(jax.random.key(seed), 9)
    return {
        "x_later": bell_draw(key_list[0], (TOKENS, D), 1.0, 6.0, ((0, 16),)),
        "kept_input_rows": bell_draw(key_list[1], (TOKENS, D), 1.0, 6.0, ((0, 16),)),
        "cotangent": gaussian_with(key_list[2], (TOKENS, D), 1.0, 8.0, ((0, 16),), (0, 1, 16, 2.0)),
        "norm_gain_vector": jnp.clip(1.0 + 0.18 * jax.random.normal(key_list[3], (D,), jnp.float32), 0.1, 1.9),
        "up_weight": bell_draw(key_list[4], (D, FF), D ** -0.5, 0.125, ((0, 8), (1, 2))),
        "down_weight": bell_draw(key_list[5], (FF, D), FF ** -0.5, 0.09375, ((0, 2), (1, 8))),
        "up_sum": bell_draw(key_list[6], (D, FF), 1.0, 6.0, ((0, 8), (1, 2)), jnp.float32),
        "down_sum": bell_draw(key_list[7], (FF, D), 1.0, 6.0, ((0, 2), (1, 8)), jnp.float32),
    }


EPSILON = 1e-06

def norm_partial_terms(values, norm_gain_vector):
    floats = values.astype(jnp.float32)
    inverse = lax.rsqrt(lax.optimization_barrier(jnp.mean(floats * floats, axis=-1, keepdims=True)) + EPSILON)
    unit_rows = floats * inverse
    normed = (unit_rows * norm_gain_vector).astype(jnp.bfloat16)
    return (inverse, unit_rows, normed)

def block_sum(left, right_weight, transpose_right):
    width = FF // N_TP
    result = jnp.zeros((left.shape[0], D), jnp.float32)
    for block in range(N_TP):
        left_block = left[:, block * width:(block + 1) * width]
        if transpose_right:
            part = jnp.dot(left_block, right_weight[:, block * width:(block + 1) * width].T, preferred_element_type=jnp.float32)
        else:
            part = jnp.dot(left_block, right_weight[block * width:(block + 1) * width], preferred_element_type=jnp.float32)
        rounded = lax.optimization_barrier(part.astype(jnp.bfloat16))
        result = result + rounded.astype(jnp.float32)
    return result

def reference(x_later, kept_input_rows, cotangent, norm_gain_vector, up_weight, down_weight, up_sum, down_sum):
    inv_later, unit_later, normed_later = norm_partial_terms(x_later, norm_gain_vector)
    inverse_rms_kept, unit_kept_rows, normed_kept_rows = norm_partial_terms(kept_input_rows, norm_gain_vector)
    pre_later = jnp.dot(normed_later, up_weight, preferred_element_type=jnp.float32)
    pre_saved = jnp.dot(normed_kept_rows, up_weight, preferred_element_type=jnp.float32)
    hidden_later = jnp.square(jax.nn.relu(pre_later)).astype(jnp.bfloat16)
    hidden_saved = jnp.square(jax.nn.relu(pre_saved)).astype(jnp.bfloat16)
    mixed = block_sum(hidden_later, down_weight, False).astype(jnp.bfloat16)
    hidden_grad = jnp.dot(cotangent, down_weight.T, preferred_element_type=jnp.float32)
    pre_grad = (hidden_grad * 2.0 * jax.nn.relu(pre_saved)).astype(jnp.bfloat16)
    normed_grad = block_sum(pre_grad, up_weight, True)
    scaled_rows = normed_grad * norm_gain_vector
    input_gradient_rows = (inverse_rms_kept * (scaled_rows - unit_kept_rows * lax.optimization_barrier(jnp.mean(scaled_rows * unit_kept_rows, axis=-1, keepdims=True)))).astype(jnp.bfloat16)
    grad_scale = TOKENS ** (-0.5)
    up_total = up_sum + grad_scale * jnp.dot(normed_kept_rows.T, pre_grad, preferred_element_type=jnp.float32)
    down_total = down_sum + grad_scale * jnp.dot(hidden_saved.T, cotangent, preferred_element_type=jnp.float32)
    return (mixed, input_gradient_rows, up_total, down_total)
```

```python
import functools

import jax
import jax.numpy as jnp
from jax import lax
from jax.experimental import pallas as pl
from jax.experimental.pallas import tpu as pltpu
from jax.sharding import PartitionSpec as P

EPSILON = 1e-06
MESH = pl.DeviceIdType.MESH
TRANSPOSED = (((1,), (1,)), ((), ()))
LEADING = (((0,), (0,)), ((), ()))
X, Y, Z = 4, 2, 1
COT, SAVED, LATER = 0, 1, 2
BACK, MIXED = 0, 1
UP, DOWN = 0, 1
VMEM_BYTES = 64 * 2**20 - 2**16


def norm_partial_terms(values, norm_gain_vector):
    floats = values.astype(jnp.float32)
    inverse = lax.rsqrt(jnp.mean(floats * floats, axis=-1, keepdims=True) + EPSILON)
    unit_rows = floats * inverse
    normed = (unit_rows * norm_gain_vector).astype(jnp.bfloat16)
    return (inverse, unit_rows, normed)


def squared_relu(pre_act):
    return jnp.square(jax.nn.relu(pre_act)).astype(jnp.bfloat16)


def body(
    x_later, kept_input_rows, cotangent, norm_gain_vector, up_weight, down_weight, up_sum, down_sum
):
    row_count = x_later.shape[0]
    grad_scale = float(row_count * lax.axis_size("rep") * lax.axis_size("fs")) ** (-0.5)
    inv_later, unit_later, normed_later = norm_partial_terms(x_later, norm_gain_vector)
    inverse_rms_kept, unit_kept_rows, normed_kept_rows = norm_partial_terms(
        kept_input_rows, norm_gain_vector
    )
    stacked = jnp.concatenate([normed_kept_rows, normed_later], axis=0)
    up_whole = lax.all_gather(up_weight, "fs", axis=0, tiled=True)
    down_whole = lax.all_gather(down_weight, "fs", axis=1, tiled=True)
    pre_act = jnp.dot(stacked, up_whole, preferred_element_type=jnp.float32)
    pre_saved = pre_act[:row_count]
    hidden_saved = squared_relu(pre_saved)
    hidden_later = squared_relu(pre_act[row_count:])
    mixed_part = jnp.dot(hidden_later, down_whole, preferred_element_type=jnp.float32)
    hidden_grad = lax.dot_general(
        cotangent, down_whole, TRANSPOSED, preferred_element_type=jnp.float32
    )
    pre_grad = (hidden_grad * 2.0 * jax.nn.relu(pre_saved)).astype(jnp.bfloat16)
    back_part = lax.dot_general(pre_grad, up_whole, TRANSPOSED, preferred_element_type=jnp.float32)
    mixed_sum, back_sum = (
        lax.psum(mixed_part.astype(jnp.bfloat16), "tp").astype(jnp.float32),
        lax.psum(back_part.astype(jnp.bfloat16), "tp").astype(jnp.float32),
    )
    mixed = mixed_sum.astype(jnp.bfloat16)
    scaled_rows = back_sum * norm_gain_vector
    input_gradient_rows = (
        inverse_rms_kept
        * (
            scaled_rows
            - unit_kept_rows * jnp.mean(scaled_rows * unit_kept_rows, axis=-1, keepdims=True)
        )
    ).astype(jnp.bfloat16)
    cot_columns, normed_columns = (
        lax.all_to_all(cotangent, "fs", split_axis=1, concat_axis=0, tiled=True),
        lax.all_to_all(normed_kept_rows, "fs", split_axis=1, concat_axis=0, tiled=True),
    )
    columns = normed_columns
    up_grad = grad_scale * lax.dot_general(
        columns,
        lax.all_gather(pre_grad, "fs", axis=0, tiled=True),
        LEADING,
        preferred_element_type=jnp.float32,
    )
    columns = cot_columns
    down_grad = lax.dot_general(
        lax.all_gather(hidden_saved, "fs", axis=0, tiled=True),
        columns,
        LEADING,
        preferred_element_type=jnp.float32,
    )
    up_added, down_added = (
        lax.psum(up_grad.astype(jnp.bfloat16), "rep").astype(jnp.float32),
        lax.psum((down_grad * grad_scale).astype(jnp.bfloat16), "rep").astype(jnp.float32),
    )
    return (mixed, input_gradient_rows, up_sum + up_added, down_sum + down_added)

def layer_kernel(
    n_fs, grad_scale, x_ref, kept_ref, cot_ref, gain_ref, up_ref, down_ref,
    mixed_out, input_out, up_out, down_out,
    tok, up_own, down_own, up_pass, down_pass, hidden, pre_grad,
    grad_kept, grad_sent, grad_got, grad_sum, grad_line, grad_pair, grad_all,
    part, got_first, got_second, got_third, rows_out,
    pair_send, pair_recv, line_send, line_recv, core_send, core_recv, own_sem,
    tok_send, tok_recv, share_send, share_recv, gline_send, gline_recv,
    gpair_send, gpair_recv, grep_send, grep_recv, part_send, part_recv, out_send, out_recv,
):
    rep, fs, core = lax.axis_index("rep"), lax.axis_index("fs"), lax.axis_index("tp")
    outer = n_fs // 2
    place, pair = fs // 2, fs % 2
    low = place % 2
    rows, width = tok.shape[2:]
    depth, own = up_pass.shape
    n_slots = tok.shape[1]
    tokens = n_slots * rows
    other_core = (rep, fs, 1 - core)
    start_row = pl.multiple_of(core * rows, rows)

    def place_at(step):
        return (place, place + 1 - 2 * low, (place + 2) % outer, outer - 1 - place)[step]

    def line_peer(step):
        return (rep, place_at(step) * 2 + pair, core)

    def partner(dim):
        if dim == X:
            return (1 - rep, fs, core)
        if dim == Y:
            return (rep, place * 2 + 1 - pair, core)
        return line_peer(1)

    def flip(bit, on):
        return 1 - bit if on else bit

    def slot(mask):
        return flip(rep, mask & X) * 4 + flip(pair, mask & Y) * 2 + flip(low, mask & Z)

    def block(rep_at, pair_at, low_at):
        return (rep_at * 2 + pair_at) * 2 + low_at

    def copy(source, target, send, recv, device):
        return pltpu.make_async_remote_copy(
            src_ref=source, dst_ref=target, send_sem=send, recv_sem=recv,
            device_id=device, device_id_type=MESH,
        )

    sent = []

    def go(source, target, send, recv, device):
        one = copy(source, target, send, recv, device)
        one.start()
        sent.append(one)

    def landed(target, sem):
        copy(target, target, sem, sem, other_core).wait_recv()

    barrier = pltpu.get_barrier_semaphore()
    peers = [other_core, partner(X), partner(Y)] + [line_peer(step) for step in range(1, outer)]
    for peer in peers:
        pl.semaphore_signal(barrier, inc=1, device_id=peer, device_id_type=MESH)

    gain = gain_ref[...]
    own_rows = pl.ds(start_row, rows)
    tok[COT, slot(0)] = cot_ref[own_rows, :]
    tok[SAVED, slot(0)] = norm_partial_terms(kept_ref[own_rows, :], gain)[2]
    tok[LATER, slot(0)] = norm_partial_terms(x_ref[own_rows, :], gain)[2]
    pl.semaphore_wait(barrier, len(peers))

    def up_source(index):
        return up_ref.at[:, pl.ds(pl.multiple_of(index * own, own), own)]

    def down_source(index):
        return down_ref.at[pl.ds(pl.multiple_of(index * own, own), own), :]

    def up_slot(half, place_to, pair_to, count=1):
        first = pl.multiple_of((place_to * 2 + pair_to) * depth, depth)
        return up_own.at[half, pl.ds(first, count * depth), :]

    def down_slot(half, place_to, pair_to, count=1):
        first = pl.multiple_of((place_to * 2 + pair_to) * depth, depth)
        return down_own.at[half, :, pl.ds(first, count * depth)]

    def send_tok(array, mask, dim):
        at = tok.at[array, slot(mask)]
        key = token_sends.setdefault((array, mask, dim), len([k for k in token_sends if k[0] == array]))
        go(at, at, tok_send.at[array, key], tok_recv.at[array, (mask ^ dim) - 1], partner(dim))

    token_sends = {}

    def tok_landed(array, mask):
        landed(tok.at[array, slot(mask)], tok_recv.at[array, mask - 1])

    orders = {COT: (Y, X), SAVED: (Y, X), LATER: (X, Y)}

    def tok_begin(array):
        for dim in (Z,) + orders[array]:
            send_tok(array, 0, dim)

    def tok_step(array, stage):
        second, third = orders[array]
        mask = (Z, second, second | Z)[stage]
        tok_landed(array, mask)
        if stage == 0:
            send_tok(array, mask, second)
        send_tok(array, mask, third)

    def tok_end(array):
        third = orders[array][1]
        for mask in (0, Z, orders[array][0], orders[array][0] | Z):
            tok_landed(array, third | mask)

    for which, low_to in enumerate((low, 1 - low)):
        index = block(rep, 1 - pair, low_to)
        up_to = up_pass if which else up_slot(core, place, pair)
        down_to = down_pass if which else down_slot(core, place, pair)
        go(up_source(index), up_to, pair_send.at[which, UP], pair_recv.at[which, UP], partner(Y))
        go(down_source(index), down_to, pair_send.at[which, DOWN], pair_recv.at[which, DOWN], partner(Y))
    for array in (COT, SAVED):
        tok_begin(array)
    keep = [
        pltpu.make_async_copy(up_source(block(rep, pair, low)), up_slot(core, place, pair), own_sem.at[UP]),
        pltpu.make_async_copy(down_source(block(rep, pair, low)), down_slot(core, place, pair), own_sem.at[DOWN]),
    ]
    for one in keep:
        one.start()
    steps = (3, 2, 1)
    for step in steps:
        index = block(rep, pair, flip(low, step % 2))
        sems = (line_send.at[step - 1, 0], line_recv.at[step - 1, 0])
        go(up_source(index), up_slot(core, place, pair), sems[0].at[UP], sems[1].at[UP], line_peer(step))
        go(down_source(index), down_slot(core, place, pair), sems[0].at[DOWN], sems[1].at[DOWN], line_peer(step))

    def to_core(step):
        at = place_at(step)
        go(
            up_slot(core, at, 0, 2), up_slot(core, at, 0, 2),
            core_send.at[step, UP], core_recv.at[step, UP], other_core,
        )
        go(
            down_slot(core, at, 0, 2), down_slot(core, at, 0, 2),
            core_send.at[step, DOWN], core_recv.at[step, DOWN], other_core,
        )

    tok_step(COT, 0)
    for which in range(2):
        landed(up_pass if which else up_slot(core, place, 1 - pair), pair_recv.at[which, UP])
        landed(down_pass if which else down_slot(core, place, 1 - pair), pair_recv.at[which, DOWN])
    for step in steps:
        up_from = up_pass if step % 2 else up_slot(core, place, 1 - pair)
        down_from = down_pass if step % 2 else down_slot(core, place, 1 - pair)
        sems = (line_send.at[step - 1, 1], line_recv.at[step - 1, 1])
        go(up_from, up_slot(core, place, 1 - pair), sems[0].at[UP], sems[1].at[UP], line_peer(step))
        go(down_from, down_slot(core, place, 1 - pair), sems[0].at[DOWN], sems[1].at[DOWN], line_peer(step))
    tok_step(SAVED, 0)
    for one in keep:
        one.wait()
    to_core(0)
    for stage in (1, 2):
        tok_step(COT, stage)
        tok_step(SAVED, stage)
    tok_begin(LATER)
    for step in (1, 2, 3):
        at = place_at(step)
        for part_of, pair_at in enumerate((pair, 1 - pair)):
            landed(up_slot(core, at, pair_at), line_recv.at[step - 1, part_of, UP])
            landed(down_slot(core, at, pair_at), line_recv.at[step - 1, part_of, DOWN])
        to_core(step)
    tok_end(COT)
    tok_end(SAVED)
    for step in range(outer):
        at = place_at(step)
        landed(up_slot(1 - core, at, 0, 2), core_recv.at[step, UP])
        landed(down_slot(1 - core, at, 0, 2), core_recv.at[step, DOWN])

    def all_tokens(array):
        return tok[array].reshape(tokens, width)

    @pl.loop(0, 2)
    def _(half):
        pre = jnp.dot(all_tokens(SAVED), up_own[half], preferred_element_type=jnp.float32)
        grad = lax.dot_general(
            all_tokens(COT), down_own[half], TRANSPOSED, preferred_element_type=jnp.float32
        )
        hidden[half] = squared_relu(pre)
        pre_grad[half] = (grad * 2.0 * jax.nn.relu(pre)).astype(jnp.bfloat16)

    tok_step(LATER, 0)

    chunk = width // outer

    def chunk_at(index):
        return pl.ds(pl.multiple_of(index * chunk, chunk), chunk)

    def weight_grad(kind, half, columns):
        left = hidden[half] if kind == DOWN else pre_grad[half]
        right = tok[COT if kind == DOWN else SAVED, :, :, columns].reshape(tokens, chunk)
        return grad_scale * lax.dot_general(left, right, LEADING, preferred_element_type=jnp.float32)

    for kind in (UP, DOWN):

        @pl.loop(0, outer)
        def _(index):
            columns = chunk_at(index)
            grad_sent[kind, :, columns] = weight_grad(kind, 1 - core, columns).astype(jnp.bfloat16)

        go(grad_sent.at[kind], grad_got.at[kind], share_send.at[kind], share_recv.at[kind], other_core)

    tok_step(LATER, 1)
    for kind in (UP, DOWN):

        @pl.loop(0, outer)
        def _(index):
            columns = chunk_at(index)
            grad_kept[kind, :, columns] = weight_grad(kind, core, columns)

    for kind in (UP, DOWN):
        landed(grad_got.at[kind], share_recv.at[kind])

        @pl.loop(0, outer)
        def _(index):
            columns = chunk_at(index)
            grad_sum[kind, :, columns] = (
                grad_kept[kind, :, columns] + grad_got[kind, :, columns].astype(jnp.float32)
            ).astype(jnp.bfloat16)

        for step in steps:
            go(
                grad_sum.at[kind, :, chunk_at(place_at(step))], grad_line.at[step - 1, kind],
                gline_send.at[step - 1, kind], gline_recv.at[step - 1, kind], line_peer(step),
            )

    @pl.loop(0, outer)
    def _(index):
        columns = chunk_at(index)
        total = jnp.zeros((tokens, chunk), jnp.float32)
        for half in range(2):
            total = total + lax.dot_general(
                pre_grad[half], up_own[half, columns, :], TRANSPOSED, preferred_element_type=jnp.float32
            )
        part[BACK, :, :, columns] = total.astype(jnp.bfloat16).reshape(n_slots, rows, chunk)

    sum_orders = {BACK: (X, Y), MIXED: (Y, X)}

    def part_first(array):
        first, second = sum_orders[array]
        for number, mask in enumerate((second | Z, second, Z, 0)):
            go(
                part.at[array, slot(first | mask)], got_first.at[array, number],
                part_send.at[array, number], part_recv.at[array, number], partner(first),
            )

    def part_add(array, mask, *got):
        total = part[array, slot(mask)].astype(jnp.float32)
        for one in got:
            total = total + one[...].astype(jnp.float32)
        return total

    def part_second(array):
        first, second = sum_orders[array]
        for number, mask in enumerate((second | Z, second)):
            landed(got_first.at[array, number], part_recv.at[array, number])
            part[array, slot(mask)] = part_add(array, mask, got_first.at[array, number]).astype(jnp.bfloat16)
            go(
                part.at[array, slot(mask)], got_second.at[array, number],
                part_send.at[array, 4 + number], part_recv.at[array, 4 + number], partner(second),
            )

    def part_third(array):
        landed(got_first.at[array, 2], part_recv.at[array, 2])
        landed(got_second.at[array, 0], part_recv.at[array, 4])
        part[array, slot(Z)] = part_add(
            array, Z, got_first.at[array, 2], got_second.at[array, 0]
        ).astype(jnp.bfloat16)
        go(
            part.at[array, slot(Z)], got_third.at[array],
            part_send.at[array, 6], part_recv.at[array, 6], partner(Z),
        )

    def part_last(array):
        landed(got_first.at[array, 3], part_recv.at[array, 3])
        landed(got_second.at[array, 1], part_recv.at[array, 5])
        landed(got_third.at[array], part_recv.at[array, 6])
        return part_add(array, 0, got_first.at[array, 3], got_second.at[array, 1], got_third.at[array])

    part_first(BACK)

    tok_step(LATER, 2)
    tok_end(LATER)

    @pl.loop(0, 2)
    def _(half):
        hidden[half] = squared_relu(
            jnp.dot(all_tokens(LATER), up_own[half], preferred_element_type=jnp.float32)
        )

    @pl.loop(0, outer)
    def _(index):
        columns = chunk_at(index)
        total = jnp.zeros((tokens, chunk), jnp.float32)
        for half in range(2):
            total = total + jnp.dot(
                hidden[half], down_own[half, :, columns], preferred_element_type=jnp.float32
            )
        part[MIXED, :, :, columns] = total.astype(jnp.bfloat16).reshape(n_slots, rows, chunk)

    part_first(MIXED)
    part_second(BACK)

    def line_part(kind, which, pair_at):
        inside = pl.ds(pl.multiple_of(pair_at * depth, depth), depth)
        if which:
            total = grad_line[0, kind, :, inside].astype(jnp.float32)
            total = total + grad_line[2, kind, :, inside].astype(jnp.float32)
        else:
            mine = pl.ds(pl.multiple_of((place * 2 + pair_at) * depth, depth), depth)
            total = grad_sum[kind, :, mine].astype(jnp.float32)
            total = total + grad_line[1, kind, :, inside].astype(jnp.float32)
        return (total.T if kind == UP else total).astype(jnp.bfloat16)

    def blocks_at(kind, rep_at, pair_at):
        return grad_all.at[kind, pl.ds(block(rep_at, pair_at, 0), 2)]

    def grad_spread(kind):
        for step in steps:
            landed(grad_line.at[step - 1, kind], gline_recv.at[step - 1, kind])
        for which, low_at in enumerate((low, 1 - low)):
            grad_pair[kind, low_at] = line_part(kind, which, 1 - pair)
        go(
            grad_pair.at[kind], blocks_at(kind, rep, pair),
            gpair_send.at[kind], gpair_recv.at[kind], partner(Y),
        )
        for which, low_at in enumerate((low, 1 - low)):
            grad_all[kind, block(rep, pair, low_at)] = line_part(kind, which, pair)
        mine = blocks_at(kind, rep, pair)
        go(mine, mine, grep_send.at[kind, 0], grep_recv.at[kind, 0], partner(X))

    def grad_pass(kind):
        near = blocks_at(kind, rep, 1 - pair)
        landed(near, gpair_recv.at[kind])
        go(near, near, grep_send.at[kind, 1], grep_recv.at[kind, 1], partner(X))

    part_third(BACK)
    grad_spread(UP)
    part_second(MIXED)
    grad_pass(UP)

    back_sum = part_last(BACK)
    inverse, unit_rows, _ = norm_partial_terms(kept_ref[own_rows, :], gain)
    scaled_rows = back_sum * gain
    rows_out[BACK, core] = (
        inverse * (scaled_rows - unit_rows * jnp.mean(scaled_rows * unit_rows, axis=-1, keepdims=True))
    ).astype(jnp.bfloat16)

    def share_rows(array):
        mine = rows_out.at[array, core]
        go(mine, mine, out_send.at[array], out_recv.at[array], other_core)

    share_rows(BACK)
    part_third(MIXED)
    grad_spread(DOWN)
    rows_out[MIXED, core] = part_last(MIXED).astype(jnp.bfloat16)
    share_rows(MIXED)
    grad_pass(DOWN)

    for array, out in ((BACK, input_out), (MIXED, mixed_out)):
        landed(rows_out.at[array, 1 - core], out_recv.at[array])
        out[...] = rows_out[array].reshape(2 * rows, width)
    for kind in (UP, DOWN):
        for number, pair_at in enumerate((pair, 1 - pair)):
            landed(blocks_at(kind, 1 - rep, pair_at), grep_recv.at[kind, number])
        for index in range(n_fs):
            if kind == UP:
                up_out[:, index * own : (index + 1) * own] = grad_all[UP, index]
            else:
                down_out[index * own : (index + 1) * own, :] = grad_all[DOWN, index]
    for one in sent:
        one.wait_send()


def cube_body(
    x_later, kept_input_rows, cotangent, norm_gain_vector, up_weight, down_weight, up_sum, down_sum
):
    row_count, width = x_later.shape
    n_fs = lax.axis_size("fs")
    grad_scale = float(row_count * lax.axis_size("rep") * n_fs) ** (-0.5)
    depth, units = up_weight.shape
    own = units // n_fs
    rows = row_count // 2
    outer = n_fs // 2
    tokens = n_fs * rows
    kind = x_later.dtype
    dma = pltpu.SemaphoreType.DMA
    vmem = functools.partial(pltpu.VMEM, dtype=kind)
    inside = pl.BlockSpec(memory_space=pltpu.VMEM)
    outside = pl.BlockSpec(memory_space=pl.ANY)
    mixed, input_gradient_rows, up_added, down_added = pl.pallas_call(
        functools.partial(layer_kernel, n_fs, grad_scale),
        out_shape=(
            jax.ShapeDtypeStruct((row_count, width), kind),
            jax.ShapeDtypeStruct((row_count, width), kind),
            jax.ShapeDtypeStruct((depth, units), kind),
            jax.ShapeDtypeStruct((units, depth), kind),
        ),
        in_specs=[inside] * 4 + [outside] * 2,
        out_specs=[inside] * 4,
        scratch_shapes=[
            vmem((3, n_fs, rows, width)),
            vmem((2, width, own)), vmem((2, own, width)), vmem((depth, own)), vmem((own, depth)),
            vmem((2, tokens, own)), vmem((2, tokens, own)),
            pltpu.VMEM((2, own, width), jnp.float32),
            vmem((2, own, width)), vmem((2, own, width)), vmem((2, own, width)),
            vmem((3, 2, own, 2 * depth)), vmem((2, 2, own, depth)), vmem((2, n_fs, own, depth)),
            vmem((2, n_fs, rows, width)),
            vmem((2, 4, rows, width)), vmem((2, 2, rows, width)), vmem((2, rows, width)),
            vmem((2, 2, rows, width)),
            dma((2, 2)), dma((2, 2)), dma((3, 2, 2)), dma((3, 2, 2)), dma((outer, 2)), dma((outer, 2)),
            dma((2,)), dma((3, 7)), dma((3, 7)), dma((2,)), dma((2,)), dma((3, 2)), dma((3, 2)),
            dma((2,)), dma((2,)), dma((2, 2)), dma((2, 2)), dma((2, 7)), dma((2, 7)), dma((2,)), dma((2,)),
        ],
        compiler_params=pltpu.CompilerParams(
            collective_id=0, has_side_effects=True, vmem_limit_bytes=VMEM_BYTES
        ),
    )(
        x_later, kept_input_rows, cotangent, norm_gain_vector.reshape(1, width), up_weight, down_weight,
    )
    return (
        mixed,
        input_gradient_rows,
        up_sum + up_added.astype(jnp.float32),
        down_sum + down_added.astype(jnp.float32),
    )


def chosen_body(*args):
    depth, units = args[4].shape
    n_fs = lax.axis_size("fs")
    cubes = lax.axis_size("tp") == 2 and lax.axis_size("rep") == 2 and n_fs == 8
    return (cube_body if cubes and units == depth * n_fs and depth % 128 == 0 else body)(*args)


def solution(mesh):
    return jax.shard_map(
        chosen_body,
        mesh=mesh,
        in_specs=(
            P(("rep", "fs"), None),
            P(("rep", "fs"), None),
            P(("rep", "fs"), None),
            P(),
            P("fs", "tp"),
            P("tp", "fs"),
            P("fs", "tp"),
            P("tp", "fs"),
        ),
        out_specs=(P(("rep", "fs"), None), P(("rep", "fs"), None), P("fs", "tp"), P("tp", "fs")),
        check_vma=False,
    )
```

```python
import functools

import jax
import jax.numpy as jnp
from jax import lax
from jax.experimental import pallas as pl
from jax.experimental.pallas import tpu as pltpu
from jax.sharding import PartitionSpec as P

EPSILON = 1e-06
MESH = pl.DeviceIdType.MESH
TRANSPOSED = (((1,), (1,)), ((), ()))
LEADING = (((0,), (0,)), ((), ()))
X, Y, Z = 4, 2, 1
COT, SAVED, LATER = 0, 1, 2
BACK, MIXED = 0, 1
UP, DOWN = 0, 1
(TOK, PAIR, LINE, LINE_PASS, CORE, PRE, GRAD, SHARE, KEEP, GRAD_LINE,
 GRAD_PAIR, GRAD_REP, BACK_SUMS, MIXED_SUMS, FIRST, SECOND, THIRD, LAST, END, TOKENS, OWN, PARTS, ROWS) = range(23)
KIND_ORDER = (DOWN, UP)
SUM_ORDERS = (((X, Y), (Y, X)), ((X, Y), (Y, X)))
SCHEDULE = (
    (TOK, COT, 0, Y), (PAIR, UP), (TOK, COT, 0, X), (TOK, SAVED, 0, Y), (TOK, LATER, 0, X),
    (TOK, SAVED, 0, Z), (LINE, UP), (TOK, SAVED, 0, X), (TOK, COT, Y, X), (TOK, COT, 0, Z),
    (TOK, SAVED, Z, Y), (PAIR, DOWN), (LINE_PASS, UP), (TOK, SAVED, Z, X), (TOK, SAVED, Y, X),
    (TOK, LATER, 0, Y), (TOK, COT, Z, Y), (CORE, UP, 0), (TOK, LATER, 0, Z), (LINE_PASS, DOWN),
    (TOK, COT, Z, X), (TOK, LATER, X, Y), (LINE, DOWN), (CORE, UP, 2), (CORE, UP, 3),
    (CORE, DOWN, 0), (CORE, UP, 1), (TOK, SAVED, Y | Z, X), (TOK, COT, Y | Z, X),
    (TOK, LATER, Z, X), (PRE, 1), (TOK, LATER, Z, Y), (PRE, 0), (CORE, DOWN, 1), (KEEP, DOWN),
    (SHARE, DOWN), (CORE, DOWN, 3), (CORE, DOWN, 2), (GRAD_LINE, DOWN), (GRAD, 0), (GRAD, 1),
    (BACK_SUMS,), (FIRST, BACK, 0, 0), (TOK, LATER, X | Z, Y), (FIRST, BACK, 0, 1),
    (FIRST, BACK, 1, 0), (MIXED_SUMS,), (SECOND, BACK, 1, 0), (KEEP, UP), (FIRST, MIXED, 0, 0),
    (SECOND, BACK, 0, 1), (FIRST, MIXED, 0, 1), (SHARE, UP), (GRAD_PAIR, DOWN, 0),
    (FIRST, MIXED, 1, 1), (SECOND, BACK, 0, 0), (SECOND, MIXED, 0, 0), (GRAD_LINE, UP),
    (FIRST, MIXED, 1, 0), (FIRST, BACK, 1, 1), (GRAD_REP, DOWN), (GRAD_PAIR, DOWN, 1),
    (THIRD, BACK, 0), (THIRD, MIXED, 0), (SECOND, BACK, 1, 1), (SECOND, MIXED, 1, 0),
    (SECOND, MIXED, 1, 1), (GRAD_PAIR, UP, 0), (GRAD_PAIR, UP, 1), (THIRD, BACK, 1), (GRAD_REP, UP),
    (THIRD, MIXED, 1), (SECOND, MIXED, 0, 1), (LAST, BACK), (LAST, MIXED), (END,),
)
VMEM_BYTES = 64 * 2**20 - 2**16


def norm_partial_terms(values, norm_gain_vector):
    floats = values.astype(jnp.float32)
    inverse = lax.rsqrt(jnp.mean(floats * floats, axis=-1, keepdims=True) + EPSILON)
    unit_rows = floats * inverse
    normed = (unit_rows * norm_gain_vector).astype(jnp.bfloat16)
    return (inverse, unit_rows, normed)


def squared_relu(pre_act):
    return jnp.square(jax.nn.relu(pre_act)).astype(jnp.bfloat16)


def body(
    x_later, kept_input_rows, cotangent, norm_gain_vector, up_weight, down_weight, up_sum, down_sum
):
    row_count = x_later.shape[0]
    grad_scale = float(row_count * lax.axis_size("rep") * lax.axis_size("fs")) ** (-0.5)
    inv_later, unit_later, normed_later = norm_partial_terms(x_later, norm_gain_vector)
    inverse_rms_kept, unit_kept_rows, normed_kept_rows = norm_partial_terms(
        kept_input_rows, norm_gain_vector
    )
    stacked = jnp.concatenate([normed_kept_rows, normed_later], axis=0)
    up_whole = lax.all_gather(up_weight, "fs", axis=0, tiled=True)
    down_whole = lax.all_gather(down_weight, "fs", axis=1, tiled=True)
    pre_act = jnp.dot(stacked, up_whole, preferred_element_type=jnp.float32)
    pre_saved = pre_act[:row_count]
    hidden_saved = squared_relu(pre_saved)
    hidden_later = squared_relu(pre_act[row_count:])
    mixed_part = jnp.dot(hidden_later, down_whole, preferred_element_type=jnp.float32)
    hidden_grad = lax.dot_general(
        cotangent, down_whole, TRANSPOSED, preferred_element_type=jnp.float32
    )
    pre_grad = (hidden_grad * 2.0 * jax.nn.relu(pre_saved)).astype(jnp.bfloat16)
    back_part = lax.dot_general(pre_grad, up_whole, TRANSPOSED, preferred_element_type=jnp.float32)
    mixed_sum, back_sum = (
        lax.psum(mixed_part.astype(jnp.bfloat16), "tp").astype(jnp.float32),
        lax.psum(back_part.astype(jnp.bfloat16), "tp").astype(jnp.float32),
    )
    mixed = mixed_sum.astype(jnp.bfloat16)
    scaled_rows = back_sum * norm_gain_vector
    input_gradient_rows = (
        inverse_rms_kept
        * (
            scaled_rows
            - unit_kept_rows * jnp.mean(scaled_rows * unit_kept_rows, axis=-1, keepdims=True)
        )
    ).astype(jnp.bfloat16)
    cot_columns, normed_columns = (
        lax.all_to_all(cotangent, "fs", split_axis=1, concat_axis=0, tiled=True),
        lax.all_to_all(normed_kept_rows, "fs", split_axis=1, concat_axis=0, tiled=True),
    )
    columns = normed_columns
    up_grad = grad_scale * lax.dot_general(
        columns,
        lax.all_gather(pre_grad, "fs", axis=0, tiled=True),
        LEADING,
        preferred_element_type=jnp.float32,
    )
    columns = cot_columns
    down_grad = lax.dot_general(
        lax.all_gather(hidden_saved, "fs", axis=0, tiled=True),
        columns,
        LEADING,
        preferred_element_type=jnp.float32,
    )
    up_added, down_added = (
        lax.psum(up_grad.astype(jnp.bfloat16), "rep").astype(jnp.float32),
        lax.psum((down_grad * grad_scale).astype(jnp.bfloat16), "rep").astype(jnp.float32),
    )
    return (mixed, input_gradient_rows, up_sum + up_added, down_sum + down_added)

def layer_kernel(
    n_fs, grad_scale, x_ref, kept_ref, cot_ref, gain_ref, up_ref, down_ref,
    mixed_out, input_out, up_out, down_out,
    kept, fresh, tok, up_own, down_own, up_pass, down_pass, pre_kept, hidden, pre_grad,
    grad_kept, grad_sent, grad_got, grad_sum, grad_line, grad_pair, grad_all,
    part, got_first, got_second, got_third, rows_out,
    load_sem, pair_send, pair_recv, line_send, line_recv, core_send, core_recv, own_sem,
    tok_send, tok_recv, share_send, share_recv, gline_send, gline_recv,
    gpair_send, gpair_recv, grep_send, grep_recv, part_send, part_recv, out_send, out_recv,
):
    rep, fs, core = lax.axis_index("rep"), lax.axis_index("fs"), lax.axis_index("tp")
    outer = n_fs // 2
    place, pair = fs // 2, fs % 2
    low = place % 2
    rows, width = tok.shape[2:]
    depth, own = up_pass.shape
    n_slots = tok.shape[1]
    tokens = n_slots * rows
    other_core = (rep, fs, 1 - core)
    start_row = pl.multiple_of(core * rows, rows)

    def place_at(step):
        return (place, place + 1 - 2 * low, (place + 2) % outer, outer - 1 - place)[step]

    def line_peer(step):
        return (rep, place_at(step) * 2 + pair, core)

    def partner(dim):
        if dim == X:
            return (1 - rep, fs, core)
        if dim == Y:
            return (rep, place * 2 + 1 - pair, core)
        return line_peer(1)

    def flip(bit, on):
        return 1 - bit if on else bit

    def slot(mask):
        return flip(rep, mask & X) * 4 + flip(pair, mask & Y) * 2 + flip(low, mask & Z)

    def block(rep_at, pair_at, low_at):
        return (rep_at * 2 + pair_at) * 2 + low_at

    def copy(source, target, send, recv, device):
        return pltpu.make_async_remote_copy(
            src_ref=source, dst_ref=target, send_sem=send, recv_sem=recv,
            device_id=device, device_id_type=MESH,
        )

    sent = []

    def go(source, target, send, recv, device):
        one = copy(source, target, send, recv, device)
        one.start()
        sent.append(one)

    seen = set()

    def landed(target, sem, *name):
        if name not in seen:
            seen.add(name)
            copy(target, target, sem, sem, other_core).wait_recv()

    own_rows = pl.ds(start_row, rows)
    loads = [
        pltpu.make_async_copy(kept_ref.at[own_rows, :], kept, load_sem.at[0]),
        pltpu.make_async_copy(x_ref.at[own_rows, :], fresh, load_sem.at[1]),
        pltpu.make_async_copy(cot_ref.at[own_rows, :], tok.at[COT, slot(0)], load_sem.at[2]),
    ]
    for one in loads:
        one.start()
    barrier = pltpu.get_barrier_semaphore()
    peers = [other_core, partner(X), partner(Y)] + [line_peer(step) for step in range(1, outer)]
    for peer in peers:
        pl.semaphore_signal(barrier, inc=1, device_id=peer, device_id_type=MESH)

    for one in loads:
        one.wait()
    gain = gain_ref[...]
    tok[SAVED, slot(0)] = norm_partial_terms(kept[...], gain)[2]
    tok[LATER, slot(0)] = norm_partial_terms(fresh[...], gain)[2]
    pl.semaphore_wait(barrier, len(peers))

    def up_source(index):
        return up_ref.at[:, pl.ds(pl.multiple_of(index * own, own), own)]

    def down_source(index):
        return down_ref.at[pl.ds(pl.multiple_of(index * own, own), own), :]

    def up_slot(half, place_to, pair_to, count=1):
        first = pl.multiple_of((place_to * 2 + pair_to) * depth, depth)
        return up_own.at[half, pl.ds(first, count * depth), :]

    def down_slot(half, place_to, pair_to, count=1):
        first = pl.multiple_of((place_to * 2 + pair_to) * depth, depth)
        return down_own.at[half, :, pl.ds(first, count * depth)]

    def tok_landed(array, mask):
        landed(tok.at[array, slot(mask)], tok_recv.at[array, mask - 1], TOKENS, array, mask)

    tok_counts = [0, 0, 0]

    def send_tok(array, mask, dim):
        if mask:
            tok_landed(array, mask)
        at = tok.at[array, slot(mask)]
        number = tok_counts[array]
        tok_counts[array] += 1
        go(at, at, tok_send.at[array, number], tok_recv.at[array, (mask ^ dim) - 1], partner(dim))

    def tok_end(array):
        for mask in range(1, n_slots):
            tok_landed(array, mask)

    sides = (UP, DOWN)
    source_of = (up_source, down_source)
    slot_of = (up_slot, down_slot)
    pass_of = (up_pass, down_pass)
    steps = (1, 3, 2)

    def pair_begin(kind):
        for which, low_to in enumerate((low, 1 - low)):
            target = pass_of[kind] if which else slot_of[kind](core, place, pair)
            go(
                source_of[kind](block(rep, 1 - pair, low_to)), target,
                pair_send.at[which, kind], pair_recv.at[which, kind], partner(Y),
            )

    def line_begin(kind):
        for step in steps:
            go(
                source_of[kind](block(rep, pair, flip(low, step % 2))), slot_of[kind](core, place, pair),
                line_send.at[step - 1, 0, kind], line_recv.at[step - 1, 0, kind], line_peer(step),
            )

    def pair_end(kind):
        landed(slot_of[kind](core, place, 1 - pair), pair_recv.at[0, kind], PAIR, kind, 0)
        landed(pass_of[kind], pair_recv.at[1, kind], PAIR, kind, 1)

    def line_pass(kind):
        pair_end(kind)
        near = slot_of[kind](core, place, 1 - pair)
        for step in steps:
            go(
                pass_of[kind] if step % 2 else near, near,
                line_send.at[step - 1, 1, kind], line_recv.at[step - 1, 1, kind], line_peer(step),
            )

    def line_landed(kind, step):
        for number, pair_at in enumerate((pair, 1 - pair)):
            landed(
                slot_of[kind](core, place_at(step), pair_at), line_recv.at[step - 1, number, kind],
                LINE, kind, step, number,
            )

    def own_end(kind):
        pair_end(kind)
        if (OWN, kind) not in seen:
            seen.add((OWN, kind))
            keep[kind].wait()

    def to_core(kind, step):
        if step:
            line_landed(kind, step)
        else:
            own_end(kind)
        mine = slot_of[kind](core, place_at(step), 0, 2)
        go(mine, mine, core_send.at[step, kind], core_recv.at[step, kind], other_core)

    def weights_end(kind, number):
        if number:
            for step in range(outer):
                target = slot_of[kind](1 - core, place_at(step), 0, 2)
                landed(target, core_recv.at[step, kind], CORE, kind, step)
        else:
            own_end(kind)
            for step in range(1, outer):
                line_landed(kind, step)

    keep = [
        pltpu.make_async_copy(
            source_of[kind](block(rep, pair, low)), slot_of[kind](core, place, pair), own_sem.at[kind]
        )
        for kind in sides
    ]

    def all_tokens(array):
        return tok[array].reshape(tokens, width)

    def saved_pre(number):
        half = (core, 1 - core)[number]
        tok_end(SAVED)
        weights_end(UP, number)
        pre = jnp.dot(all_tokens(SAVED), up_own[half], preferred_element_type=jnp.float32)
        pre_kept[half] = jax.nn.relu(pre)
        hidden[half] = squared_relu(pre)

    def saved_grad(number):
        half = (core, 1 - core)[number]
        tok_end(COT)
        weights_end(DOWN, number)
        grad = lax.dot_general(
            all_tokens(COT), down_own[half], TRANSPOSED, preferred_element_type=jnp.float32
        )
        pre_grad[half] = (grad * 2.0 * pre_kept[half]).astype(jnp.bfloat16)

    chunk = width // outer

    def chunk_at(index):
        return pl.ds(pl.multiple_of(index * chunk, chunk), chunk)

    def weight_grad(kind, half, columns):
        left = hidden[half] if kind == DOWN else pre_grad[half]
        right = tok[COT if kind == DOWN else SAVED, :, :, columns].reshape(tokens, chunk)
        return grad_scale * lax.dot_general(left, right, LEADING, preferred_element_type=jnp.float32)

    def grad_share(kind):
        if kind == DOWN:
            tok_end(COT)

        @pl.loop(0, outer)
        def _(index):
            columns = chunk_at(index)
            grad_sent[kind, :, columns] = weight_grad(kind, 1 - core, columns).astype(jnp.bfloat16)

        go(grad_sent.at[kind], grad_got.at[kind], share_send.at[kind], share_recv.at[kind], other_core)

    def grad_keep(kind):
        if kind == DOWN:
            tok_end(COT)

        @pl.loop(0, outer)
        def _(index):
            columns = chunk_at(index)
            grad_kept[kind, :, columns] = weight_grad(kind, core, columns)

    def grad_begin(kind):
        landed(grad_got.at[kind], share_recv.at[kind], SHARE, kind)

        @pl.loop(0, outer)
        def _(index):
            columns = chunk_at(index)
            grad_sum[kind, :, columns] = (
                grad_kept[kind, :, columns] + grad_got[kind, :, columns].astype(jnp.float32)
            ).astype(jnp.bfloat16)

        for number, pair_at in enumerate((1 - pair, pair)):
            for step in steps:
                columns = pl.ds(pl.multiple_of((place_at(step) * 2 + pair_at) * depth, depth), depth)
                go(
                    grad_sum.at[kind, :, columns], grad_line.at[step - 1, kind, number],
                    gline_send.at[step - 1, kind, number], gline_recv.at[step - 1, kind, number],
                    line_peer(step),
                )

    def part_at(array, side, mask):
        return part.at[array, slot(mask), side]

    def part_first(array, side, number):
        first, second = SUM_ORDERS[array][side]
        for place_in in (2 * number, 2 * number + 1):
            mask = (second | Z, second, Z, 0)[place_in]
            go(
                part_at(array, side, first | mask), got_first.at[array, side, place_in],
                part_send.at[array, side, place_in], part_recv.at[array, side, place_in], partner(first),
            )

    def part_landed(array, side, number):
        got = got_first.at[array, side, number] if number < 4 else (
            got_second.at[array, side, number - 4] if number < 6 else got_third.at[array, side]
        )
        landed(got, part_recv.at[array, side, number], PARTS, array, side, number)
        return got

    def part_add(array, side, mask, *got):
        total = part_at(array, side, mask)[...].astype(jnp.float32)
        for one in got:
            total = total + one[...].astype(jnp.float32)
        return total

    def part_second(array, side, number):
        first, second = SUM_ORDERS[array][side]
        mask = (second | Z, second)[number]
        got = part_landed(array, side, number)
        at = part_at(array, side, mask)
        at[...] = part_add(array, side, mask, got).astype(jnp.bfloat16)
        go(
            at, got_second.at[array, side, number],
            part_send.at[array, side, 4 + number], part_recv.at[array, side, 4 + number], partner(second),
        )

    def part_third(array, side):
        got = [part_landed(array, side, number) for number in (2, 4)]
        at = part_at(array, side, Z)
        at[...] = part_add(array, side, Z, *got).astype(jnp.bfloat16)
        go(
            at, got_third.at[array, side],
            part_send.at[array, side, 6], part_recv.at[array, side, 6], partner(Z),
        )

    def part_last(array, side):
        return part_add(array, side, 0, *[part_landed(array, side, number) for number in (3, 5, 6)])

    def back_sums():
        @pl.loop(0, outer)
        def _(index):
            columns = chunk_at(index)
            total = jnp.zeros((tokens, chunk), jnp.float32)
            for half in range(2):
                total = total + lax.dot_general(
                    pre_grad[half], up_own[half, columns, :], TRANSPOSED,
                    preferred_element_type=jnp.float32,
                )
            part[BACK, :, :, :, columns] = total.astype(jnp.bfloat16).reshape(n_slots, 2, rows // 2, chunk)

    def mixed_sums():
        tok_end(LATER)

        @pl.loop(0, 2)
        def _(half):
            hidden[half] = squared_relu(
                jnp.dot(all_tokens(LATER), up_own[half], preferred_element_type=jnp.float32)
            )

        @pl.loop(0, outer)
        def _(index):
            columns = chunk_at(index)
            total = jnp.zeros((tokens, chunk), jnp.float32)
            for half in range(2):
                total = total + jnp.dot(
                    hidden[half], down_own[half, :, columns], preferred_element_type=jnp.float32
                )
            part[MIXED, :, :, :, columns] = total.astype(jnp.bfloat16).reshape(n_slots, 2, rows // 2, chunk)

    def line_part(kind, which, number):
        if which:
            total = grad_line[0, kind, number].astype(jnp.float32)
            total = total + grad_line[2, kind, number].astype(jnp.float32)
        else:
            pair_at = (1 - pair, pair)[number]
            mine = pl.ds(pl.multiple_of((place * 2 + pair_at) * depth, depth), depth)
            total = grad_sum[kind, :, mine].astype(jnp.float32)
            total = total + grad_line[1, kind, number].astype(jnp.float32)
        return (total.T if kind == UP else total).astype(jnp.bfloat16)

    def blocks_at(kind, rep_at, pair_at):
        return grad_all.at[kind, pl.ds(block(rep_at, pair_at, 0), 2)]

    def grad_spread(kind, number):
        for step in steps:
            landed(
                grad_line.at[step - 1, kind, number], gline_recv.at[step - 1, kind, number],
                GRAD_LINE, kind, step, number,
            )
        for which, low_at in enumerate((low, 1 - low)):
            if number:
                grad_all[kind, block(rep, pair, low_at)] = line_part(kind, which, number)
            else:
                grad_pair[kind, low_at] = line_part(kind, which, number)
        mine = blocks_at(kind, rep, pair)
        if number:
            go(mine, mine, grep_send.at[kind, 0], grep_recv.at[kind, 0], partner(X))
            grad_out(kind, rep, pair)
        else:
            go(grad_pair.at[kind], mine, gpair_send.at[kind], gpair_recv.at[kind], partner(Y))

    def grad_pass(kind):
        near = blocks_at(kind, rep, 1 - pair)
        landed(near, gpair_recv.at[kind], GRAD_PAIR, kind)
        go(near, near, grep_send.at[kind, 1], grep_recv.at[kind, 1], partner(X))
        grad_out(kind, rep, 1 - pair)

    def grad_out(kind, rep_at, pair_at):
        for low_at in range(2):
            index = block(rep_at, pair_at, low_at)
            place_to = pl.ds(pl.multiple_of(index * own, own), own)
            if kind == UP:
                up_out[:, place_to] = grad_all[UP, index]
            else:
                down_out[place_to, :] = grad_all[DOWN, index]

    def grad_end(kind, number):
        pair_at = (pair, 1 - pair)[number]
        landed(blocks_at(kind, 1 - rep, pair_at), grep_recv.at[kind, number], GRAD_REP, kind, number)
        grad_out(kind, 1 - rep, pair_at)

    def share_rows(array):
        mine = rows_out.at[array, core]
        go(mine, mine, out_send.at[array], out_recv.at[array], other_core)

    def back_end():
        for side in range(2):
            scaled_rows = part_last(BACK, side) * gain
            at = pl.ds(side * (rows // 2), rows // 2)
            inverse, unit_rows, _ = norm_partial_terms(kept[at, :], gain)
            rows_out[BACK, core, side] = (
                inverse
                * (scaled_rows - unit_rows * jnp.mean(scaled_rows * unit_rows, axis=-1, keepdims=True))
            ).astype(jnp.bfloat16)
        share_rows(BACK)

    def mixed_end():
        for side in range(2):
            rows_out[MIXED, core, side] = part_last(MIXED, side).astype(jnp.bfloat16)
        share_rows(MIXED)

    def rows_end(array, out):
        landed(rows_out.at[array, 1 - core], out_recv.at[array], ROWS, array)
        out[...] = rows_out[array].reshape(2 * rows, width)

    def finish():
        for kind in KIND_ORDER:
            for number in range(2):
                grad_end(kind, number)
        rows_end(BACK, input_out)
        rows_end(MIXED, mixed_out)

    for one in keep:
        one.start()
    ends = (back_end, mixed_end)
    jobs = {
        TOK: send_tok, PAIR: pair_begin, LINE: line_begin, LINE_PASS: line_pass, CORE: to_core,
        PRE: saved_pre, GRAD: saved_grad, SHARE: grad_share, KEEP: grad_keep, GRAD_LINE: grad_begin,
        GRAD_PAIR: grad_spread, GRAD_REP: grad_pass, BACK_SUMS: back_sums, MIXED_SUMS: mixed_sums,
        FIRST: part_first, SECOND: part_second, THIRD: part_third, LAST: lambda array: ends[array](),
        END: finish,
    }
    for job, *details in SCHEDULE:
        jobs[job](*details)
    for one in sent:
        one.wait_send()


def cube_body(
    x_later, kept_input_rows, cotangent, norm_gain_vector, up_weight, down_weight, up_sum, down_sum
):
    row_count, width = x_later.shape
    n_fs = lax.axis_size("fs")
    grad_scale = float(row_count * lax.axis_size("rep") * n_fs) ** (-0.5)
    depth, units = up_weight.shape
    own = units // n_fs
    rows = row_count // 2
    outer = n_fs // 2
    tokens = n_fs * rows
    kind = x_later.dtype
    dma = pltpu.SemaphoreType.DMA
    vmem = functools.partial(pltpu.VMEM, dtype=kind)
    inside = pl.BlockSpec(memory_space=pltpu.VMEM)
    outside = pl.BlockSpec(memory_space=pltpu.HBM)
    mixed, input_gradient_rows, up_added, down_added = pl.pallas_call(
        functools.partial(layer_kernel, n_fs, grad_scale),
        out_shape=(
            jax.ShapeDtypeStruct((row_count, width), kind),
            jax.ShapeDtypeStruct((row_count, width), kind),
            jax.ShapeDtypeStruct((depth, units), kind),
            jax.ShapeDtypeStruct((units, depth), kind),
        ),
        in_specs=[outside] * 3 + [inside] + [outside] * 2,
        out_specs=[inside] * 4,
        scratch_shapes=[
            vmem((rows, width)), vmem((rows, width)), vmem((3, n_fs, rows, width)),
            vmem((2, width, own)), vmem((2, own, width)), vmem((depth, own)), vmem((own, depth)),
            pltpu.VMEM((2, tokens, own), jnp.float32), vmem((2, tokens, own)), vmem((2, tokens, own)),
            pltpu.VMEM((2, own, width), jnp.float32),
            vmem((2, own, width)), vmem((2, own, width)), vmem((2, own, width)),
            vmem((3, 2, 2, own, depth)), vmem((2, 2, own, depth)), vmem((2, n_fs, own, depth)),
            vmem((2, n_fs, 2, rows // 2, width)),
            vmem((2, 2, 4, rows // 2, width)), vmem((2, 2, 2, rows // 2, width)),
            vmem((2, 2, rows // 2, width)), vmem((2, 2, 2, rows // 2, width)),
            dma((3,)), dma((2, 2)), dma((2, 2)), dma((3, 2, 2)), dma((3, 2, 2)), dma((outer, 2)), dma((outer, 2)),
            dma((2,)), dma((3, 7)), dma((3, 7)), dma((2,)), dma((2,)), dma((3, 2, 2)), dma((3, 2, 2)),
            dma((2,)), dma((2,)), dma((2, 2)), dma((2, 2)), dma((2, 2, 7)), dma((2, 2, 7)), dma((2,)), dma((2,)),
        ],
        compiler_params=pltpu.CompilerParams(
            collective_id=0, has_side_effects=True, vmem_limit_bytes=VMEM_BYTES
        ),
    )(
        x_later, kept_input_rows, cotangent, norm_gain_vector.reshape(1, width), up_weight, down_weight,
    )
    return (
        mixed,
        input_gradient_rows,
        up_sum + up_added.astype(jnp.float32),
        down_sum + down_added.astype(jnp.float32),
    )


def chosen_body(*args):
    depth, units = args[4].shape
    n_fs = lax.axis_size("fs")
    cubes = lax.axis_size("tp") == 2 and lax.axis_size("rep") == 2 and n_fs == 8
    return (cube_body if cubes and units == depth * n_fs and depth % 128 == 0 else body)(*args)


def solution(mesh):
    return jax.shard_map(
        chosen_body,
        mesh=mesh,
        in_specs=(
            P(("rep", "fs"), None),
            P(("rep", "fs"), None),
            P(("rep", "fs"), None),
            P(),
            P("fs", "tp"),
            P("tp", "fs"),
            P("fs", "tp"),
            P("tp", "fs"),
        ),
        out_specs=(P(("rep", "fs"), None), P(("rep", "fs"), None), P("fs", "tp"), P("tp", "fs")),
        check_vma=False,
    )
```

```python
import functools

import jax
import jax.numpy as jnp
from jax import lax
from jax.experimental import pallas as pl
from jax.experimental.pallas import tpu as pltpu
from jax.sharding import PartitionSpec as P

EPSILON = 1e-06
MESH = pl.DeviceIdType.MESH
TRANSPOSED = (((1,), (1,)), ((), ()))
LEADING = (((0,), (0,)), ((), ()))
X, Y, Z = 4, 2, 1
COT, SAVED, LATER = 0, 1, 2
BACK, MIXED = 0, 1
UP, DOWN = 0, 1
(TOK, PAIR, LINE, LINE_PASS, CORE, PRE, GRAD, SHARE, KEEP, GRAD_LINE,
 GRAD_PAIR, GRAD_REP, BACK_SUMS, MIXED_SUMS, FIRST, SECOND, THIRD, LAST, END, TOKENS, OWN, PARTS, ROWS) = range(23)
KIND_ORDER = (DOWN, UP)
TOKEN_ORDERS = (((Z, X, Y), (Z, Y, X)), ((Z, Y, X), (Z, Y, X)), ((Z, X, Y), (Z, Y, X)))
SUM_ORDERS = (((Y, X, Z), (X, Y, Z)), ((Y, X, Z), (Y, X, Z)))
SCHEDULE = (
    (TOK, COT, 1, 1), (TOK, COT, 0, 0), (TOK, COT, 0, 1), (TOK, SAVED, 0, 2), (TOK, SAVED, 1, 1),
    (TOK, SAVED, 1, 0), (TOK, LATER, 0, 1), (LINE, UP), (TOK, LATER, 1, 1), (TOK, COT, 1, 5),
    (TOK, SAVED, 1, 2), (PAIR, UP), (TOK, COT, 1, 2), (TOK, SAVED, 0, 0), (CORE, UP, 0),
    (TOK, COT, 1, 0), (TOK, SAVED, 0, 1), (TOK, LATER, 0, 0), (LINE_PASS, UP), (TOK, LATER, 1, 5),
    (TOK, SAVED, 0, 3), (TOK, COT, 0, 4), (LINE, DOWN), (TOK, SAVED, 1, 4), (TOK, SAVED, 1, 3),
    (TOK, LATER, 1, 0), (TOK, COT, 0, 3), (TOK, COT, 0, 5), (TOK, SAVED, 0, 5), (TOK, SAVED, 1, 5),
    (PAIR, DOWN), (TOK, COT, 1, 3), (TOK, SAVED, 1, 6), (TOK, SAVED, 0, 4), (CORE, UP, 2),
    (TOK, COT, 0, 2), (CORE, UP, 1), (TOK, SAVED, 0, 6), (TOK, COT, 0, 6), (CORE, UP, 3),
    (TOK, COT, 1, 6), (CORE, DOWN, 0), (TOK, COT, 1, 4), (TOK, LATER, 0, 4), (LINE_PASS, DOWN),
    (TOK, LATER, 0, 5), (TOK, LATER, 1, 3), (TOK, LATER, 1, 2), (TOK, LATER, 0, 2), (PRE, 1),
    (PRE, 0), (SHARE, DOWN), (TOK, LATER, 0, 3), (TOK, LATER, 1, 4), (KEEP, DOWN),
    (GRAD_LINE, DOWN), (CORE, DOWN, 1), (CORE, DOWN, 3), (TOK, LATER, 0, 6), (CORE, DOWN, 2),
    (GRAD, 0), (TOK, LATER, 1, 6), (GRAD, 1), (BACK_SUMS,), (FIRST, BACK, 1, 1),
    (FIRST, BACK, 0, 1), (KEEP, UP), (SHARE, UP), (FIRST, BACK, 1, 0), (FIRST, BACK, 0, 0),
    (SECOND, BACK, 0, 0), (GRAD_PAIR, DOWN, 0), (SECOND, BACK, 0, 1), (MIXED_SUMS,),
    (FIRST, MIXED, 0, 0), (GRAD_LINE, UP), (FIRST, MIXED, 0, 1), (GRAD_PAIR, DOWN, 1),
    (FIRST, MIXED, 1, 0), (GRAD_REP, DOWN), (SECOND, MIXED, 0, 1), (SECOND, BACK, 1, 0),
    (SECOND, MIXED, 1, 0), (SECOND, MIXED, 0, 0), (GRAD_PAIR, UP, 0), (SECOND, MIXED, 1, 1),
    (THIRD, BACK, 1), (GRAD_PAIR, UP, 1), (THIRD, BACK, 0), (FIRST, MIXED, 1, 1), (THIRD, MIXED, 0),
    (GRAD_REP, UP), (THIRD, MIXED, 1), (SECOND, BACK, 1, 1), (LAST, MIXED), (LAST, BACK), (END,),
)
VMEM_BYTES = 48 * 2**20


def norm_partial_terms(values, norm_gain_vector):
    floats = values.astype(jnp.float32)
    inverse = lax.rsqrt(jnp.mean(floats * floats, axis=-1, keepdims=True) + EPSILON)
    unit_rows = floats * inverse
    normed = (unit_rows * norm_gain_vector).astype(jnp.bfloat16)
    return (inverse, unit_rows, normed)


def squared_relu(pre_act):
    return jnp.square(jax.nn.relu(pre_act)).astype(jnp.bfloat16)


def body(
    x_later, kept_input_rows, cotangent, norm_gain_vector, up_weight, down_weight, up_sum, down_sum
):
    row_count = x_later.shape[0]
    grad_scale = float(row_count * lax.axis_size("rep") * lax.axis_size("fs")) ** (-0.5)
    inv_later, unit_later, normed_later = norm_partial_terms(x_later, norm_gain_vector)
    inverse_rms_kept, unit_kept_rows, normed_kept_rows = norm_partial_terms(
        kept_input_rows, norm_gain_vector
    )
    stacked = jnp.concatenate([normed_kept_rows, normed_later], axis=0)
    up_whole = lax.all_gather(up_weight, "fs", axis=0, tiled=True)
    down_whole = lax.all_gather(down_weight, "fs", axis=1, tiled=True)
    pre_act = jnp.dot(stacked, up_whole, preferred_element_type=jnp.float32)
    pre_saved = pre_act[:row_count]
    hidden_saved = squared_relu(pre_saved)
    hidden_later = squared_relu(pre_act[row_count:])
    mixed_part = jnp.dot(hidden_later, down_whole, preferred_element_type=jnp.float32)
    hidden_grad = lax.dot_general(
        cotangent, down_whole, TRANSPOSED, preferred_element_type=jnp.float32
    )
    pre_grad = (hidden_grad * 2.0 * jax.nn.relu(pre_saved)).astype(jnp.bfloat16)
    back_part = lax.dot_general(pre_grad, up_whole, TRANSPOSED, preferred_element_type=jnp.float32)
    mixed_sum, back_sum = (
        lax.psum(mixed_part.astype(jnp.bfloat16), "tp").astype(jnp.float32),
        lax.psum(back_part.astype(jnp.bfloat16), "tp").astype(jnp.float32),
    )
    mixed = mixed_sum.astype(jnp.bfloat16)
    scaled_rows = back_sum * norm_gain_vector
    input_gradient_rows = (
        inverse_rms_kept
        * (
            scaled_rows
            - unit_kept_rows * jnp.mean(scaled_rows * unit_kept_rows, axis=-1, keepdims=True)
        )
    ).astype(jnp.bfloat16)
    cot_columns, normed_columns = (
        lax.all_to_all(cotangent, "fs", split_axis=1, concat_axis=0, tiled=True),
        lax.all_to_all(normed_kept_rows, "fs", split_axis=1, concat_axis=0, tiled=True),
    )
    columns = normed_columns
    up_grad = grad_scale * lax.dot_general(
        columns,
        lax.all_gather(pre_grad, "fs", axis=0, tiled=True),
        LEADING,
        preferred_element_type=jnp.float32,
    )
    columns = cot_columns
    down_grad = lax.dot_general(
        lax.all_gather(hidden_saved, "fs", axis=0, tiled=True),
        columns,
        LEADING,
        preferred_element_type=jnp.float32,
    )
    up_added, down_added = (
        lax.psum(up_grad.astype(jnp.bfloat16), "rep").astype(jnp.float32),
        lax.psum((down_grad * grad_scale).astype(jnp.bfloat16), "rep").astype(jnp.float32),
    )
    return (mixed, input_gradient_rows, up_sum + up_added, down_sum + down_added)

def layer_kernel(
    n_fs, grad_scale, x_ref, kept_ref, cot_ref, gain_ref, up_ref, down_ref, up_sum_ref, down_sum_ref,
    mixed_out, input_out, up_out, down_out,
    gain_kept, kept, fresh, tok, up_own, down_own, up_pass, down_pass, pre_kept, hidden, pre_grad,
    grad_kept, grad_sent, grad_got, grad_sum, grad_line, grad_pair, grad_all,
    part, got_first, got_second, got_third, rows_out, up_total, down_total,
    load_sem, pair_send, pair_recv, line_send, line_recv, core_send, core_recv, own_sem,
    tok_send, tok_recv, tok_last, share_send, share_recv, gline_send, gline_recv,
    gpair_send, gpair_recv, grep_send, grep_recv, part_send, part_recv, part_end,
    out_send, out_recv, sum_sem, store_sem,
):
    rep, fs, core = lax.axis_index("rep"), lax.axis_index("fs"), lax.axis_index("tp")
    outer = n_fs // 2
    place, pair = fs // 2, fs % 2
    low = place % 2
    half_rows, width = tok.shape[3:]
    rows = 2 * half_rows
    depth, own = up_pass.shape
    n_slots = tok.shape[1]
    tokens = n_slots * rows
    other_core = (rep, fs, 1 - core)
    start_row = pl.multiple_of(core * rows, rows)

    def place_at(step):
        return (place, place + 1 - 2 * low, (place + 2) % outer, outer - 1 - place)[step]

    def line_peer(step):
        return (rep, place_at(step) * 2 + pair, core)

    def partner(dim):
        if dim == X:
            return (1 - rep, fs, core)
        if dim == Y:
            return (rep, place * 2 + 1 - pair, core)
        return line_peer(1)

    def flip(bit, on):
        return 1 - bit if on else bit

    def slot(mask):
        return flip(rep, mask & X) * 4 + flip(pair, mask & Y) * 2 + flip(low, mask & Z)

    def block(rep_at, pair_at, low_at):
        return (rep_at * 2 + pair_at) * 2 + low_at

    def copy(source, target, send, recv, device):
        return pltpu.make_async_remote_copy(
            src_ref=source, dst_ref=target, send_sem=send, recv_sem=recv,
            device_id=device, device_id_type=MESH,
        )

    def reached(order, reach):
        return sum(dim for step, dim in enumerate(order) if reach >> step & 1)

    def go(source, target, send, recv, device):
        copy(source, target, send, recv, device).start()

    def all_sent(source, sem):
        copy(source, source, sem, sem, other_core).wait_send()

    seen = set()

    def landed(target, sem, *name):
        if name not in seen:
            seen.add(name)
            copy(target, target, sem, sem, other_core).wait_recv()

    own_rows = pl.ds(start_row, rows)
    loads = [
        pltpu.make_async_copy(kept_ref.at[own_rows, :], kept, load_sem.at[0]),
        pltpu.make_async_copy(x_ref.at[own_rows, :], fresh, load_sem.at[1]),
    ]
    loads += [
        pltpu.make_async_copy(
            cot_ref.at[pl.ds(pl.multiple_of(start_row + side * half_rows, half_rows), half_rows), :],
            tok.at[COT, slot(0), side], load_sem.at[2 + side],
        )
        for side in range(2)
    ]
    loads += [
        pltpu.make_async_copy(gain_ref, gain_kept, load_sem.at[4]),
    ]
    for one in loads:
        one.start()
    barrier = pltpu.get_barrier_semaphore()
    peers = [other_core, partner(X), partner(Y)] + [line_peer(step) for step in range(1, outer)]
    for peer in peers:
        pl.semaphore_signal(barrier, inc=1, device_id=peer, device_id_type=MESH)

    for one in loads:
        one.wait()
    gain = gain_kept[...]
    own_shape = (2, half_rows, width)
    tok[SAVED, slot(0)] = norm_partial_terms(kept[...], gain)[2].reshape(own_shape)
    tok[LATER, slot(0)] = norm_partial_terms(fresh[...], gain)[2].reshape(own_shape)
    pl.semaphore_wait(barrier, len(peers))

    def up_source(index):
        return up_ref.at[:, pl.ds(pl.multiple_of(index * own, own), own)]

    def down_source(index):
        return down_ref.at[pl.ds(pl.multiple_of(index * own, own), own), :]

    def up_slot(half, place_to, pair_to, count=1):
        first = pl.multiple_of((place_to * 2 + pair_to) * depth, depth)
        return up_own.at[half, pl.ds(first, count * depth), :]

    def down_slot(half, place_to, pair_to, count=1):
        first = pl.multiple_of((place_to * 2 + pair_to) * depth, depth)
        return down_own.at[half, :, pl.ds(first, count * depth)]

    def tok_landed(array, side, reach):
        mask = reached(TOKEN_ORDERS[array][side], reach)
        landed(tok.at[array, slot(mask), side], tok_recv.at[array, side, reach - 1], TOKENS, array, side, reach)

    def send_tok(array, side, number):
        reach, step = ((0, 0), (0, 1), (0, 2), (1, 1), (1, 2), (2, 2), (3, 2))[number]
        order = TOKEN_ORDERS[array][side]
        if reach:
            tok_landed(array, side, reach)
        at = tok.at[array, slot(reached(order, reach)), side]
        recv = tok_last.at[array] if step == 2 else tok_recv.at[array, side, (reach | 1 << step) - 1]
        go(at, at, tok_send.at[0], recv, partner(order[step]))

    def tok_end(array):
        for side in range(2):
            for reach in (1, 2, 3):
                tok_landed(array, side, reach)
        landed(tok.at[array, : n_slots // 2], tok_last.at[array], TOKENS, array)

    sides = (UP, DOWN)
    source_of = (up_source, down_source)
    slot_of = (up_slot, down_slot)
    pass_of = (up_pass, down_pass)
    steps = (1, 3, 2)

    def pair_begin(kind):
        for which, low_to in enumerate((low, 1 - low)):
            target = pass_of[kind] if which else slot_of[kind](core, place, pair)
            go(
                source_of[kind](block(rep, 1 - pair, low_to)), target,
                pair_send.at[0], pair_recv.at[kind], partner(Y),
            )

    def line_begin(kind):
        for step in steps:
            go(
                source_of[kind](block(rep, pair, flip(low, step % 2))), slot_of[kind](core, place, pair),
                line_send.at[0], line_recv.at[step - 1, kind], line_peer(step),
            )

    def pair_end(kind):
        landed(slot_of[kind](core, place, 0, 2), pair_recv.at[kind], PAIR, kind)

    def line_pass(kind):
        pair_end(kind)
        near = slot_of[kind](core, place, 1 - pair)
        for step in steps:
            go(
                pass_of[kind] if step % 2 else near, near,
                line_send.at[0], line_recv.at[step - 1, kind], line_peer(step),
            )

    def line_landed(kind, step):
        landed(slot_of[kind](core, place_at(step), 0, 2), line_recv.at[step - 1, kind], LINE, kind, step)

    def own_end(kind):
        pair_end(kind)
        if (OWN, kind) not in seen:
            seen.add((OWN, kind))
            keep[kind].wait()

    def to_core(kind, step):
        if step:
            line_landed(kind, step)
        else:
            own_end(kind)
        mine = slot_of[kind](core, place_at(step), 0, 2)
        go(mine, mine, core_send.at[0], core_recv.at[kind], other_core)

    def weights_end(kind, number):
        if number:
            landed((up_own, down_own)[kind].at[1 - core], core_recv.at[kind], CORE, kind)
        else:
            own_end(kind)
            for step in range(1, outer):
                line_landed(kind, step)

    keep = [
        pltpu.make_async_copy(
            source_of[kind](block(rep, pair, low)), slot_of[kind](core, place, pair), own_sem.at[kind]
        )
        for kind in sides
    ]

    def all_tokens(array):
        return tok[array].reshape(tokens, width)

    def saved_pre(number):
        half = (core, 1 - core)[number]
        tok_end(SAVED)
        weights_end(UP, number)
        pre = jnp.dot(all_tokens(SAVED), up_own[half], preferred_element_type=jnp.float32)
        pre_kept[half] = jax.nn.relu(pre)
        hidden[half] = squared_relu(pre)

    def saved_grad(number):
        half = (core, 1 - core)[number]
        tok_end(COT)
        weights_end(DOWN, number)
        grad = lax.dot_general(
            all_tokens(COT), down_own[half], TRANSPOSED, preferred_element_type=jnp.float32
        )
        pre_grad[half] = (grad * 2.0 * pre_kept[half]).astype(jnp.bfloat16)

    chunk = width // outer

    def chunk_at(index):
        return pl.ds(pl.multiple_of(index * chunk, chunk), chunk)

    def weight_grad(kind, half, columns):
        left = hidden[half] if kind == DOWN else pre_grad[half]
        right = tok[COT if kind == DOWN else SAVED, :, :, :, columns].reshape(tokens, chunk)
        return grad_scale * lax.dot_general(left, right, LEADING, preferred_element_type=jnp.float32)

    def grad_share(kind):
        if kind == DOWN:
            tok_end(COT)

        @pl.loop(0, outer)
        def _(index):
            columns = chunk_at(index)
            grad_sent[kind, :, columns] = weight_grad(kind, 1 - core, columns).astype(jnp.bfloat16)

        go(grad_sent.at[kind], grad_got.at[kind], share_send.at[0], share_recv.at[kind], other_core)

    def grad_keep(kind):
        if kind == DOWN:
            tok_end(COT)

        @pl.loop(0, outer)
        def _(index):
            columns = chunk_at(index)
            grad_kept[kind, :, columns] = weight_grad(kind, core, columns)

    def grad_begin(kind):
        landed(grad_got.at[kind], share_recv.at[kind], SHARE, kind)

        @pl.loop(0, outer)
        def _(index):
            columns = chunk_at(index)
            grad_sum[kind, :, columns] = (
                grad_kept[kind, :, columns] + grad_got[kind, :, columns].astype(jnp.float32)
            ).astype(jnp.bfloat16)

        for number, pair_at in enumerate((1 - pair, pair)):
            for step in steps:
                columns = pl.ds(pl.multiple_of((place_at(step) * 2 + pair_at) * depth, depth), depth)
                go(
                    grad_sum.at[kind, :, columns], grad_line.at[step - 1, kind, number],
                    gline_send.at[0], gline_recv.at[kind, number], line_peer(step),
                )

    def part_at(array, side, mask):
        return part.at[array, slot(mask), side]

    def part_mask(array, side, number):
        first, second, third = SUM_ORDERS[array][side]
        return (second | third, second, third, 0, third, 0)[number]

    def part_first(array, side, number):
        first = SUM_ORDERS[array][side][0]
        for place_in in (2 * number, 2 * number + 1):
            go(
                part_at(array, side, first | part_mask(array, side, place_in)),
                got_first.at[array, side, place_in],
                part_send.at[0], part_sem(array, side, place_in), partner(first),
            )

    def part_sem(array, side, number):
        if number in (3, 5, 6):
            return part_end.at[array]
        return part_recv.at[array, side, min(number, 2)]

    def part_add(array, side, mask, *got):
        total = part_at(array, side, mask)[...].astype(jnp.float32)
        for one in got:
            total = total + one[...].astype(jnp.float32)
        return total

    def part_second(array, side, number):
        mask = part_mask(array, side, number)
        got = got_first.at[array, side, number]
        landed(got, part_sem(array, side, number), SECOND, array, side, number)
        at = part_at(array, side, mask)
        at[...] = part_add(array, side, mask, got).astype(jnp.bfloat16)
        go(
            at, got_second.at[array, side, number],
            part_send.at[0], part_sem(array, side, 4 + number), partner(SUM_ORDERS[array][side][1]),
        )

    def part_third(array, side):
        third = SUM_ORDERS[array][side][2]
        got = (got_first.at[array, side, 2], got_second.at[array, side, 0])
        landed(got_second.at[array, side], part_sem(array, side, 2), THIRD, array, side)
        at = part_at(array, side, third)
        at[...] = part_add(array, side, third, *got).astype(jnp.bfloat16)
        go(
            at, got_third.at[array, side],
            part_send.at[0], part_sem(array, side, 6), partner(third),
        )

    def part_last(array, side):
        landed(part.at[array, : n_slots // 2 - 1], part_end.at[array], LAST, array, PARTS)
        return part_add(
            array, side, 0,
            got_first.at[array, side, 3], got_second.at[array, side, 1], got_third.at[array, side],
        )

    def back_sums():
        @pl.loop(0, outer)
        def _(index):
            columns = chunk_at(index)
            total = jnp.zeros((tokens, chunk), jnp.float32)
            for half in range(2):
                total = total + lax.dot_general(
                    pre_grad[half], up_own[half, columns, :], TRANSPOSED,
                    preferred_element_type=jnp.float32,
                )
            part[BACK, :, :, :, columns] = total.astype(jnp.bfloat16).reshape(n_slots, 2, rows // 2, chunk)

    def mixed_sums():
        tok_end(LATER)

        @pl.loop(0, 2)
        def _(half):
            hidden[half] = squared_relu(
                jnp.dot(all_tokens(LATER), up_own[half], preferred_element_type=jnp.float32)
            )

        @pl.loop(0, outer)
        def _(index):
            columns = chunk_at(index)
            total = jnp.zeros((tokens, chunk), jnp.float32)
            for half in range(2):
                total = total + jnp.dot(
                    hidden[half], down_own[half, :, columns], preferred_element_type=jnp.float32
                )
            part[MIXED, :, :, :, columns] = total.astype(jnp.bfloat16).reshape(n_slots, 2, rows // 2, chunk)

    def line_part(kind, which, number):
        if which:
            total = grad_line[0, kind, number].astype(jnp.float32)
            total = total + grad_line[2, kind, number].astype(jnp.float32)
        else:
            pair_at = (1 - pair, pair)[number]
            mine = pl.ds(pl.multiple_of((place * 2 + pair_at) * depth, depth), depth)
            total = grad_sum[kind, :, mine].astype(jnp.float32)
            total = total + grad_line[1, kind, number].astype(jnp.float32)
        return (total.T if kind == UP else total).astype(jnp.bfloat16)

    def blocks_at(kind, rep_at, pair_at):
        return grad_all.at[kind, pl.ds(block(rep_at, pair_at, 0), 2)]

    def grad_spread(kind, number):
        landed(grad_line.at[:, kind, number], gline_recv.at[kind, number], GRAD_LINE, kind, number)
        for which, low_at in enumerate((low, 1 - low)):
            if number:
                grad_all[kind, block(rep, pair, low_at)] = line_part(kind, which, number)
            else:
                grad_pair[kind, low_at] = line_part(kind, which, number)
        mine = blocks_at(kind, rep, pair)
        if number:
            go(mine, mine, grep_send.at[0], grep_recv.at[kind, 0], partner(X))
            grad_out(kind, rep, pair)
        else:
            go(grad_pair.at[kind], mine, gpair_send.at[0], gpair_recv.at[kind], partner(Y))

    def grad_pass(kind):
        near = blocks_at(kind, rep, 1 - pair)
        landed(near, gpair_recv.at[kind], GRAD_PAIR, kind)
        go(near, near, grep_send.at[0], grep_recv.at[kind, 1], partner(X))
        grad_out(kind, rep, 1 - pair)

    def store(source, target, number):
        pltpu.make_async_copy(source, target, store_sem.at[number]).start()

    def grad_out(kind, rep_at, pair_at):
        if (ROWS, kind) not in seen:
            seen.add((ROWS, kind))
            sums[kind].wait()
        for low_at in range(2):
            index = block(rep_at, pair_at, low_at)
            place_to = pl.ds(pl.multiple_of(index * own, own), own)
            if kind == UP:
                up_total[:, place_to] += grad_all[UP, index].astype(jnp.float32)
            else:
                down_total[place_to, :] += grad_all[DOWN, index].astype(jnp.float32)
        first = pl.ds(pl.multiple_of(block(rep_at, pair_at, 0) * own, own), 2 * own)
        at = (slice(None), first) if kind == UP else (first, slice(None))
        store((up_total, down_total)[kind].at[at], (up_out, down_out)[kind].at[at], kind)

    def grad_end(kind, number):
        pair_at = (pair, 1 - pair)[number]
        landed(blocks_at(kind, 1 - rep, pair_at), grep_recv.at[kind, number], GRAD_REP, kind, number)
        grad_out(kind, 1 - rep, pair_at)

    def share_rows(array):
        mine = rows_out.at[array, core]
        go(mine, mine, out_send.at[0], out_recv.at[array], other_core)
        store(mine, (input_out, mixed_out)[array].at[core], 2)

    def back_end():
        for side in range(2):
            scaled_rows = part_last(BACK, side) * gain
            at = pl.ds(side * (rows // 2), rows // 2)
            inverse, unit_rows, _ = norm_partial_terms(kept[at, :], gain)
            rows_out[BACK, core, side] = (
                inverse
                * (scaled_rows - unit_rows * jnp.mean(scaled_rows * unit_rows, axis=-1, keepdims=True))
            ).astype(jnp.bfloat16)
        share_rows(BACK)

    def mixed_end():
        for side in range(2):
            rows_out[MIXED, core, side] = part_last(MIXED, side).astype(jnp.bfloat16)
        share_rows(MIXED)

    def rows_end(array, out):
        landed(rows_out.at[array, 1 - core], out_recv.at[array], LAST, array)
        store(rows_out.at[array, 1 - core], out.at[1 - core], 2)

    def finish():
        for kind in KIND_ORDER:
            for number in range(2):
                grad_end(kind, number)
        rows_end(BACK, input_out)
        rows_end(MIXED, mixed_out)
        for number, whole in enumerate((up_total, down_total, rows_out)):
            pltpu.make_async_copy(whole, whole, store_sem.at[number]).wait()
        all_sent(tok.at[:, 1:], tok_send.at[0])
        all_sent(part.at[:, 1:], part_send.at[0])
        all_sent(up_own.at[:, : 3 * width // 4], line_send.at[0])
        all_sent(grad_sum.at[:, :, : 3 * width // 4], gline_send.at[0])
        all_sent(up_own.at[0, : width // 2], pair_send.at[0])
        all_sent(up_own, core_send.at[0])
        all_sent(grad_sent, share_send.at[0])
        all_sent(grad_pair, gpair_send.at[0])
        all_sent(grad_all.at[:, : n_fs // 2], grep_send.at[0])
        all_sent(rows_out.at[:, 0], out_send.at[0])

    sums = [
        pltpu.make_async_copy(up_sum_ref, up_total, sum_sem.at[UP]),
        pltpu.make_async_copy(down_sum_ref, down_total, sum_sem.at[DOWN]),
    ]
    for one in keep + sums:
        one.start()
    ends = (back_end, mixed_end)
    jobs = {
        TOK: send_tok, PAIR: pair_begin, LINE: line_begin, LINE_PASS: line_pass, CORE: to_core,
        PRE: saved_pre, GRAD: saved_grad, SHARE: grad_share, KEEP: grad_keep, GRAD_LINE: grad_begin,
        GRAD_PAIR: grad_spread, GRAD_REP: grad_pass, BACK_SUMS: back_sums, MIXED_SUMS: mixed_sums,
        FIRST: part_first, SECOND: part_second, THIRD: part_third, LAST: lambda array: ends[array](),
        END: finish,
    }
    for job, *details in SCHEDULE:
        jobs[job](*details)


def store_kernel(*refs):
    count = len(refs) // 2
    copies = [
        pltpu.make_async_copy(refs[index], refs[count + index], refs[-1].at[index])
        for index in range(count)
    ]
    for one in copies:
        one.start()
    for one in copies:
        one.wait()


def cube_body(
    x_later, kept_input_rows, cotangent, norm_gain_vector, up_weight, down_weight, up_sum, down_sum
):
    row_count, width = x_later.shape
    n_fs = lax.axis_size("fs")
    grad_scale = float(row_count * lax.axis_size("rep") * n_fs) ** (-0.5)
    depth, units = up_weight.shape
    own = units // n_fs
    rows = row_count // 2
    outer = n_fs // 2
    tokens = n_fs * rows
    kind = x_later.dtype
    dma = pltpu.SemaphoreType.DMA
    vmem = functools.partial(pltpu.VMEM, dtype=kind)
    outside = pl.BlockSpec(memory_space=pltpu.HBM)
    results = pl.pallas_call(
        functools.partial(layer_kernel, n_fs, grad_scale),
        out_shape=(
            jax.ShapeDtypeStruct((2, 2, rows // 2, width), kind),
            jax.ShapeDtypeStruct((2, 2, rows // 2, width), kind),
            jax.ShapeDtypeStruct((depth, units), jnp.float32),
            jax.ShapeDtypeStruct((units, depth), jnp.float32),
        ),
        in_specs=[outside] * 8,
        out_specs=[pl.BlockSpec(memory_space=pl.ANY)] * 4,
        scratch_shapes=[
            pltpu.VMEM((1, width), jnp.float32), vmem((rows, width)), vmem((rows, width)), vmem((3, n_fs, 2, rows // 2, width)),
            vmem((2, width, own)), vmem((2, own, width)), vmem((depth, own)), vmem((own, depth)),
            pltpu.VMEM((2, tokens, own), jnp.float32), vmem((2, tokens, own)), vmem((2, tokens, own)),
            pltpu.VMEM((2, own, width), jnp.float32),
            vmem((2, own, width)), vmem((2, own, width)), vmem((2, own, width)),
            vmem((3, 2, 2, own, depth)), vmem((2, 2, own, depth)), vmem((2, n_fs, own, depth)),
            vmem((2, n_fs, 2, rows // 2, width)),
            vmem((2, 2, 4, rows // 2, width)), vmem((2, 2, 2, rows // 2, width)),
            vmem((2, 2, rows // 2, width)), vmem((2, 2, 2, rows // 2, width)),
            pltpu.VMEM((depth, units), jnp.float32), pltpu.VMEM((units, depth), jnp.float32),
            dma((5,)), dma((1,)), dma((2,)), dma((1,)), dma((3, 2)), dma((1,)), dma((2,)), dma((2,)),
            dma((1,)), dma((3, 2, 3)), dma((3,)), dma((1,)), dma((2,)), dma((1,)), dma((2, 2)),
            dma((1,)), dma((2,)), dma((1,)), dma((2, 2)), dma((1,)), dma((2, 2, 3)), dma((2,)),
            dma((1,)), dma((2,)), dma((2,)), dma((3,)),
        ],
        compiler_params=pltpu.CompilerParams(
            collective_id=0, has_side_effects=True, vmem_limit_bytes=VMEM_BYTES
        ),
    )(
        *[
            pltpu.with_memory_space_constraint(values, pltpu.HBM)
            for values in (
                x_later, kept_input_rows, cotangent, norm_gain_vector.reshape(1, width),
                up_weight, down_weight, up_sum, down_sum,
            )
        ],
    )
    results = [one.reshape(row_count, width) for one in results[:2]] + list(results[2:])
    return pl.pallas_call(
        store_kernel,
        out_shape=[jax.ShapeDtypeStruct(one.shape, one.dtype) for one in results],
        in_specs=[pl.BlockSpec(memory_space=pl.ANY)] * len(results),
        out_specs=[pl.BlockSpec(memory_space=pl.ANY)] * len(results),
        scratch_shapes=[dma((len(results),))],
        compiler_params=pltpu.CompilerParams(vmem_limit_bytes=2**20),
    )(*results)


def chosen_body(*args):
    depth, units = args[4].shape
    n_fs = lax.axis_size("fs")
    cubes = lax.axis_size("tp") == 2 and lax.axis_size("rep") == 2 and n_fs == 8
    return (cube_body if cubes and units == depth * n_fs and depth % 128 == 0 else body)(*args)


def solution(mesh):
    return jax.shard_map(
        chosen_body,
        mesh=mesh,
        in_specs=(
            P(("rep", "fs"), None),
            P(("rep", "fs"), None),
            P(("rep", "fs"), None),
            P(),
            P("fs", "tp"),
            P("tp", "fs"),
            P("fs", "tp"),
            P("tp", "fs"),
        ),
        out_specs=(P(("rep", "fs"), None), P(("rep", "fs"), None), P("fs", "tp"), P("tp", "fs")),
        check_vma=False,
    )
```

```python
import functools

import jax
import jax.numpy as jnp
from jax import lax
from jax.experimental import pallas as pl
from jax.experimental.pallas import tpu as pltpu
from jax.sharding import PartitionSpec as P

EPSILON = 1e-06
MESH = pl.DeviceIdType.MESH
TRANSPOSED = (((1,), (1,)), ((), ()))
LEADING = (((0,), (0,)), ((), ()))
X, Y, Z = 4, 2, 1
COT, SAVED, LATER = 0, 1, 2
BACK, MIXED = 0, 1
UP, DOWN = 0, 1
(TOK, PAIR, LINE, LINE_PASS, CORE, PRE, GRAD, SHARE, KEEP, GRAD_LINE,
 GRAD_PAIR, GRAD_REP, BACK_SUMS, MIXED_SUMS, FIRST, SECOND, THIRD, LAST, END, GRAD_GO, TOKENS, OWN, PARTS, ROWS) = range(24)
KIND_ORDER = (DOWN, UP)
TOKEN_ORDERS = (((Z, Y, X), (Z, X, Y)), ((Z, Y, X), (Z, Y, X)), ((Z, Y, X), (Z, X, Y)))
SUM_ORDERS = (((Y, X, Z), (X, Z, Y)), ((Y, X, Z), (Y, Z, X)))
SCHEDULE = (
    (TOK, COT, 0, 2), (TOK, SAVED, 1, 1), (TOK, COT, 1, 1), (TOK, COT, 0, 1), (TOK, SAVED, 1, 2),
    (LINE, DOWN, 2), (PAIR, UP), (TOK, COT, 1, 0), (PAIR, DOWN), (TOK, SAVED, 1, 5),
    (TOK, LATER, 1, 1), (TOK, SAVED, 0, 0), (TOK, COT, 1, 5), (LINE, UP, 2), (TOK, COT, 1, 3),
    (TOK, SAVED, 0, 1), (TOK, LATER, 1, 2), (TOK, SAVED, 1, 0), (LINE_PASS, UP, 3),
    (TOK, COT, 0, 0), (TOK, COT, 0, 5), (TOK, SAVED, 0, 4), (TOK, SAVED, 1, 3), (TOK, SAVED, 1, 4),
    (TOK, COT, 1, 6), (TOK, SAVED, 0, 3), (LINE, UP, 1), (LINE_PASS, UP, 2), (CORE, DOWN, 0),
    (LINE_PASS, UP, 1), (TOK, SAVED, 0, 2), (LINE_PASS, DOWN, 2), (TOK, LATER, 1, 0),
    (TOK, SAVED, 1, 6), (LINE, UP, 3), (TOK, COT, 0, 4), (TOK, COT, 0, 3), (TOK, COT, 1, 2),
    (TOK, LATER, 0, 0), (TOK, SAVED, 0, 5), (TOK, SAVED, 0, 6), (TOK, COT, 1, 4), (TOK, COT, 0, 6),
    (TOK, LATER, 1, 5), (LINE_PASS, DOWN, 1), (CORE, UP, 2), (LINE, DOWN, 3), (TOK, LATER, 1, 3),
    (TOK, LATER, 0, 3), (CORE, UP, 0), (CORE, UP, 3), (TOK, LATER, 0, 1), (TOK, LATER, 1, 4),
    (CORE, UP, 1), (PRE, 0), (LINE, DOWN, 1), (CORE, DOWN, 2), (LINE_PASS, DOWN, 3), (PRE, 1),
    (SHARE, DOWN), (TOK, LATER, 0, 4), (KEEP, DOWN), (TOK, LATER, 0, 2), (GRAD_LINE, DOWN),
    (GRAD_GO, DOWN, 0, 2), (TOK, LATER, 0, 6), (GRAD_GO, DOWN, 0, 1), (CORE, DOWN, 1),
    (GRAD_GO, DOWN, 0, 3), (TOK, LATER, 1, 6), (CORE, DOWN, 3), (GRAD_GO, DOWN, 1, 1), (GRAD, 0),
    (TOK, LATER, 0, 5), (GRAD, 1), (BACK_SUMS, 0), (FIRST, BACK, 0, 0), (BACK_SUMS, 1),
    (FIRST, BACK, 1, 1), (MIXED_SUMS, 1), (FIRST, MIXED, 1, 0), (GRAD_GO, DOWN, 1, 2),
    (FIRST, BACK, 1, 0), (MIXED_SUMS, 0), (SHARE, UP), (KEEP, UP), (GRAD_LINE, UP),
    (GRAD_GO, UP, 0, 1), (SECOND, MIXED, 1, 0), (FIRST, MIXED, 0, 0), (GRAD_GO, UP, 0, 3),
    (GRAD_GO, UP, 1, 1), (GRAD_PAIR, DOWN, 0), (GRAD_GO, UP, 0, 2), (SECOND, BACK, 0, 0),
    (SECOND, BACK, 0, 1), (GRAD_GO, DOWN, 1, 3), (SECOND, MIXED, 0, 0), (FIRST, MIXED, 1, 1),
    (SECOND, MIXED, 0, 1), (GRAD_REP, DOWN), (GRAD_PAIR, UP, 0), (GRAD_GO, UP, 1, 3),
    (SECOND, BACK, 1, 0), (FIRST, MIXED, 0, 1), (THIRD, MIXED, 1), (GRAD_PAIR, DOWN, 1),
    (SECOND, BACK, 1, 1), (GRAD_GO, UP, 1, 2), (GRAD_REP, UP), (SECOND, MIXED, 1, 1),
    (THIRD, MIXED, 0), (FIRST, BACK, 0, 1), (GRAD_PAIR, UP, 1), (THIRD, BACK, 1), (THIRD, BACK, 0),
    (LAST, MIXED), (LAST, BACK), (END,),
)
VMEM_BYTES = 48 * 2**20


def norm_partial_terms(values, norm_gain_vector):
    floats = values.astype(jnp.float32)
    inverse = lax.rsqrt(jnp.mean(floats * floats, axis=-1, keepdims=True) + EPSILON)
    unit_rows = floats * inverse
    normed = (unit_rows * norm_gain_vector).astype(jnp.bfloat16)
    return (inverse, unit_rows, normed)


def squared_relu(pre_act):
    return jnp.square(jax.nn.relu(pre_act)).astype(jnp.bfloat16)


def body(
    x_later, kept_input_rows, cotangent, norm_gain_vector, up_weight, down_weight, up_sum, down_sum
):
    row_count = x_later.shape[0]
    grad_scale = float(row_count * lax.axis_size("rep") * lax.axis_size("fs")) ** (-0.5)
    inv_later, unit_later, normed_later = norm_partial_terms(x_later, norm_gain_vector)
    inverse_rms_kept, unit_kept_rows, normed_kept_rows = norm_partial_terms(
        kept_input_rows, norm_gain_vector
    )
    stacked = jnp.concatenate([normed_kept_rows, normed_later], axis=0)
    up_whole = lax.all_gather(up_weight, "fs", axis=0, tiled=True)
    down_whole = lax.all_gather(down_weight, "fs", axis=1, tiled=True)
    pre_act = jnp.dot(stacked, up_whole, preferred_element_type=jnp.float32)
    pre_saved = pre_act[:row_count]
    hidden_saved = squared_relu(pre_saved)
    hidden_later = squared_relu(pre_act[row_count:])
    mixed_part = jnp.dot(hidden_later, down_whole, preferred_element_type=jnp.float32)
    hidden_grad = lax.dot_general(
        cotangent, down_whole, TRANSPOSED, preferred_element_type=jnp.float32
    )
    pre_grad = (hidden_grad * 2.0 * jax.nn.relu(pre_saved)).astype(jnp.bfloat16)
    back_part = lax.dot_general(pre_grad, up_whole, TRANSPOSED, preferred_element_type=jnp.float32)
    mixed_sum, back_sum = (
        lax.psum(mixed_part.astype(jnp.bfloat16), "tp").astype(jnp.float32),
        lax.psum(back_part.astype(jnp.bfloat16), "tp").astype(jnp.float32),
    )
    mixed = mixed_sum.astype(jnp.bfloat16)
    scaled_rows = back_sum * norm_gain_vector
    input_gradient_rows = (
        inverse_rms_kept
        * (
            scaled_rows
            - unit_kept_rows * jnp.mean(scaled_rows * unit_kept_rows, axis=-1, keepdims=True)
        )
    ).astype(jnp.bfloat16)
    cot_columns, normed_columns = (
        lax.all_to_all(cotangent, "fs", split_axis=1, concat_axis=0, tiled=True),
        lax.all_to_all(normed_kept_rows, "fs", split_axis=1, concat_axis=0, tiled=True),
    )
    columns = normed_columns
    up_grad = grad_scale * lax.dot_general(
        columns,
        lax.all_gather(pre_grad, "fs", axis=0, tiled=True),
        LEADING,
        preferred_element_type=jnp.float32,
    )
    columns = cot_columns
    down_grad = lax.dot_general(
        lax.all_gather(hidden_saved, "fs", axis=0, tiled=True),
        columns,
        LEADING,
        preferred_element_type=jnp.float32,
    )
    up_added, down_added = (
        lax.psum(up_grad.astype(jnp.bfloat16), "rep").astype(jnp.float32),
        lax.psum((down_grad * grad_scale).astype(jnp.bfloat16), "rep").astype(jnp.float32),
    )
    return (mixed, input_gradient_rows, up_sum + up_added, down_sum + down_added)

def layer_kernel(
    n_fs, grad_scale, x_ref, kept_ref, cot_ref, gain_ref, up_ref, down_ref, up_sum_ref, down_sum_ref,
    mixed_out, input_out, up_out, down_out,
    gain_kept, kept, fresh, tok, up_own, down_own, up_pass, down_pass, pre_kept, hidden, pre_grad,
    grad_kept, grad_sent, grad_got, grad_sum, grad_line, grad_pair, grad_all,
    part, got_first, got_second, got_third, rows_out, up_total, down_total,
    load_sem, pair_send, pair_recv, line_send, line_recv, core_send, core_recv, own_sem,
    tok_send, tok_recv, tok_last, share_send, share_recv, gline_send, gline_recv,
    gpair_send, gpair_recv, grep_send, grep_recv, part_send, part_recv, part_end,
    out_send, out_recv, sum_sem, store_sem,
):
    rep, fs, core = lax.axis_index("rep"), lax.axis_index("fs"), lax.axis_index("tp")
    outer = n_fs // 2
    place, pair = fs // 2, fs % 2
    low = place % 2
    half_rows, width = tok.shape[3:]
    rows = 2 * half_rows
    depth, own = up_pass.shape
    n_slots = tok.shape[1]
    tokens = n_slots * rows
    other_core = (rep, fs, 1 - core)
    start_row = pl.multiple_of(core * rows, rows)

    def place_at(step):
        return (place, place + 1 - 2 * low, (place + 2) % outer, outer - 1 - place)[step]

    def line_peer(step):
        return (rep, place_at(step) * 2 + pair, core)

    def partner(dim):
        if dim == X:
            return (1 - rep, fs, core)
        if dim == Y:
            return (rep, place * 2 + 1 - pair, core)
        return line_peer(1)

    def flip(bit, on):
        return 1 - bit if on else bit

    def slot(mask):
        return flip(rep, mask & X) * 4 + flip(pair, mask & Y) * 2 + flip(low, mask & Z)

    def block(rep_at, pair_at, low_at):
        return (rep_at * 2 + pair_at) * 2 + low_at

    def copy(source, target, send, recv, device):
        return pltpu.make_async_remote_copy(
            src_ref=source, dst_ref=target, send_sem=send, recv_sem=recv,
            device_id=device, device_id_type=MESH,
        )

    def reached(order, reach):
        return sum(dim for step, dim in enumerate(order) if reach >> step & 1)

    def go(source, target, send, recv, device):
        copy(source, target, send, recv, device).start()

    def all_sent(source, sem):
        copy(source, source, sem, sem, other_core).wait_send()

    seen = set()

    def landed(target, sem, *name):
        if name not in seen:
            seen.add(name)
            copy(target, target, sem, sem, other_core).wait_recv()

    own_rows = pl.ds(start_row, rows)
    loads = [
        pltpu.make_async_copy(kept_ref.at[own_rows, :], kept, load_sem.at[0]),
        pltpu.make_async_copy(x_ref.at[own_rows, :], fresh, load_sem.at[1]),
    ]
    loads += [
        pltpu.make_async_copy(
            cot_ref.at[pl.ds(pl.multiple_of(start_row + side * half_rows, half_rows), half_rows), :],
            tok.at[COT, slot(0), side], load_sem.at[2 + side],
        )
        for side in range(2)
    ]
    loads += [
        pltpu.make_async_copy(gain_ref, gain_kept, load_sem.at[4]),
    ]
    for one in loads:
        one.start()
    barrier = pltpu.get_barrier_semaphore()
    peers = [other_core, partner(X), partner(Y)] + [line_peer(step) for step in range(1, outer)]
    for peer in peers:
        pl.semaphore_signal(barrier, inc=1, device_id=peer, device_id_type=MESH)

    for one in loads:
        one.wait()
    gain = gain_kept[...]
    own_shape = (2, half_rows, width)
    tok[SAVED, slot(0)] = norm_partial_terms(kept[...], gain)[2].reshape(own_shape)
    tok[LATER, slot(0)] = norm_partial_terms(fresh[...], gain)[2].reshape(own_shape)
    pl.semaphore_wait(barrier, len(peers))

    def up_source(index):
        return up_ref.at[:, pl.ds(pl.multiple_of(index * own, own), own)]

    def down_source(index):
        return down_ref.at[pl.ds(pl.multiple_of(index * own, own), own), :]

    def up_slot(half, place_to, pair_to, count=1):
        first = pl.multiple_of((place_to * 2 + pair_to) * depth, depth)
        return up_own.at[half, pl.ds(first, count * depth), :]

    def down_slot(half, place_to, pair_to, count=1):
        first = pl.multiple_of((place_to * 2 + pair_to) * depth, depth)
        return down_own.at[half, :, pl.ds(first, count * depth)]

    def tok_landed(array, side, reach):
        mask = reached(TOKEN_ORDERS[array][side], reach)
        landed(tok.at[array, slot(mask), side], tok_recv.at[array, side, reach - 1], TOKENS, array, side, reach)

    def send_tok(array, side, number):
        reach, step = ((0, 0), (0, 1), (0, 2), (1, 1), (1, 2), (2, 2), (3, 2))[number]
        order = TOKEN_ORDERS[array][side]
        if reach:
            tok_landed(array, side, reach)
        at = tok.at[array, slot(reached(order, reach)), side]
        recv = tok_last.at[array, side] if step == 2 else tok_recv.at[array, side, (reach | 1 << step) - 1]
        go(at, at, tok_send.at[0], recv, partner(order[step]))

    def tok_end(array, which=(0, 1)):
        for side in which:
            for reach in (1, 2, 3):
                tok_landed(array, side, reach)
            landed(tok.at[array, : n_slots // 2, side], tok_last.at[array, side], TOKENS, array, side)

    sides = (UP, DOWN)
    source_of = (up_source, down_source)
    slot_of = (up_slot, down_slot)
    pass_of = (up_pass, down_pass)

    def pair_begin(kind):
        for which, low_to in enumerate((low, 1 - low)):
            target = pass_of[kind] if which else slot_of[kind](core, place, pair)
            go(
                source_of[kind](block(rep, 1 - pair, low_to)), target,
                pair_send.at[0], pair_recv.at[kind], partner(Y),
            )

    def line_begin(kind, step):
        go(
            source_of[kind](block(rep, pair, flip(low, step % 2))), slot_of[kind](core, place, pair),
            line_send.at[0], line_recv.at[step - 1, kind], line_peer(step),
        )

    def pair_end(kind):
        landed(slot_of[kind](core, place, 0, 2), pair_recv.at[kind], PAIR, kind)

    def line_pass(kind, step):
        pair_end(kind)
        near = slot_of[kind](core, place, 1 - pair)
        go(
            pass_of[kind] if step % 2 else near, near,
            line_send.at[0], line_recv.at[step - 1, kind], line_peer(step),
        )

    def line_landed(kind, step):
        landed(slot_of[kind](core, place_at(step), 0, 2), line_recv.at[step - 1, kind], LINE, kind, step)

    def own_end(kind):
        pair_end(kind)
        if (OWN, kind) not in seen:
            seen.add((OWN, kind))
            keep[kind].wait()

    def to_core(kind, step):
        if step:
            line_landed(kind, step)
        else:
            own_end(kind)
        mine = slot_of[kind](core, place_at(step), 0, 2)
        go(mine, mine, core_send.at[0], core_recv.at[kind], other_core)

    def weights_end(kind, number):
        if number:
            landed((up_own, down_own)[kind].at[1 - core], core_recv.at[kind], CORE, kind)
        else:
            own_end(kind)
            for step in range(1, outer):
                line_landed(kind, step)

    keep = [
        pltpu.make_async_copy(
            source_of[kind](block(rep, pair, low)), slot_of[kind](core, place, pair), own_sem.at[kind]
        )
        for kind in sides
    ]

    def all_tokens(array):
        return tok[array].reshape(tokens, width)

    def saved_pre(number):
        half = (core, 1 - core)[number]
        tok_end(SAVED)
        weights_end(UP, number)
        pre = jnp.dot(all_tokens(SAVED), up_own[half], preferred_element_type=jnp.float32)
        pre_kept[half] = jax.nn.relu(pre)
        hidden[half] = squared_relu(pre).reshape(hidden.shape[1:])

    def saved_grad(number):
        half = (core, 1 - core)[number]
        tok_end(COT)
        weights_end(DOWN, number)
        grad = lax.dot_general(
            all_tokens(COT), down_own[half], TRANSPOSED, preferred_element_type=jnp.float32
        )
        pre_grad[half] = (grad * 2.0 * pre_kept[half]).astype(jnp.bfloat16).reshape(pre_grad.shape[1:])

    chunk = width // outer

    def chunk_at(index):
        return pl.ds(pl.multiple_of(index * chunk, chunk), chunk)

    def weight_grad(kind, half, columns):
        left = (hidden[half] if kind == DOWN else pre_grad[half]).reshape(tokens, own)
        right = tok[COT if kind == DOWN else SAVED, :, :, :, columns].reshape(tokens, chunk)
        return grad_scale * lax.dot_general(left, right, LEADING, preferred_element_type=jnp.float32)

    def grad_share(kind):
        if kind == DOWN:
            tok_end(COT)

        @pl.loop(0, outer)
        def _(index):
            columns = chunk_at(index)
            grad_sent[kind, :, columns] = weight_grad(kind, 1 - core, columns).astype(jnp.bfloat16)

        go(grad_sent.at[kind], grad_got.at[kind], share_send.at[0], share_recv.at[kind], other_core)

    def grad_keep(kind):
        if kind == DOWN:
            tok_end(COT)

        @pl.loop(0, outer)
        def _(index):
            columns = chunk_at(index)
            grad_kept[kind, :, columns] = weight_grad(kind, core, columns)

    def grad_begin(kind):
        landed(grad_got.at[kind], share_recv.at[kind], SHARE, kind)

        @pl.loop(0, outer)
        def _(index):
            columns = chunk_at(index)
            grad_sum[kind, :, columns] = (
                grad_kept[kind, :, columns] + grad_got[kind, :, columns].astype(jnp.float32)
            ).astype(jnp.bfloat16)

    def grad_go(kind, number, step):
        pair_at = (1 - pair, pair)[number]
        columns = pl.ds(pl.multiple_of((place_at(step) * 2 + pair_at) * depth, depth), depth)
        go(
            grad_sum.at[kind, :, columns], grad_line.at[step - 1, kind, number],
            gline_send.at[0], gline_recv.at[kind, number], line_peer(step),
        )

    def part_at(array, side, mask):
        return part.at[array, slot(mask), side]

    def part_mask(array, side, number):
        first, second, third = SUM_ORDERS[array][side]
        return (second | third, second, third, 0, third, 0)[number]

    def part_first(array, side, number):
        first = SUM_ORDERS[array][side][0]
        for place_in in (2 * number, 2 * number + 1):
            go(
                part_at(array, side, first | part_mask(array, side, place_in)),
                got_first.at[array, side, place_in],
                part_send.at[0], part_sem(array, side, place_in), partner(first),
            )

    def part_sem(array, side, number):
        if number in (3, 5, 6):
            return part_end.at[array]
        return part_recv.at[array, side, min(number, 2)]

    def part_add(array, side, mask, *got):
        total = part_at(array, side, mask)[...].astype(jnp.float32)
        for one in got:
            total = total + one[...].astype(jnp.float32)
        return total

    def part_second(array, side, number):
        mask = part_mask(array, side, number)
        got = got_first.at[array, side, number]
        landed(got, part_sem(array, side, number), SECOND, array, side, number)
        at = part_at(array, side, mask)
        at[...] = part_add(array, side, mask, got).astype(jnp.bfloat16)
        go(
            at, got_second.at[array, side, number],
            part_send.at[0], part_sem(array, side, 4 + number), partner(SUM_ORDERS[array][side][1]),
        )

    def part_third(array, side):
        third = SUM_ORDERS[array][side][2]
        got = (got_first.at[array, side, 2], got_second.at[array, side, 0])
        landed(got_second.at[array, side], part_sem(array, side, 2), THIRD, array, side)
        at = part_at(array, side, third)
        at[...] = part_add(array, side, third, *got).astype(jnp.bfloat16)
        go(
            at, got_third.at[array, side],
            part_send.at[0], part_sem(array, side, 6), partner(third),
        )

    def part_last(array, side):
        landed(part.at[array, : n_slots // 2 - 1], part_end.at[array], LAST, array, PARTS)
        return part_add(
            array, side, 0,
            got_first.at[array, side, 3], got_second.at[array, side, 1], got_third.at[array, side],
        )

    def side_of(ref, side):
        return ref[:, side].reshape(tokens // 2, ref.shape[-1])

    def store_part(array, side, columns, total):
        part[array, :, side, :, columns] = total.astype(jnp.bfloat16).reshape(n_slots, half_rows, chunk)

    def back_sums(side):
        @pl.loop(0, outer)
        def _(index):
            columns = chunk_at(index)
            total = jnp.zeros((tokens // 2, chunk), jnp.float32)
            for half in range(2):
                total = total + lax.dot_general(
                    side_of(pre_grad.at[half], side), up_own[half, columns, :], TRANSPOSED,
                    preferred_element_type=jnp.float32,
                )
            store_part(BACK, side, columns, total)

    def mixed_sums(side):
        tok_end(LATER, (side,))

        @pl.loop(0, 2)
        def _(half):
            hidden[half, :, side] = squared_relu(
                jnp.dot(
                    side_of(tok.at[LATER], side), up_own[half], preferred_element_type=jnp.float32
                )
            ).reshape(n_slots, half_rows, own)

        @pl.loop(0, outer)
        def _(index):
            columns = chunk_at(index)
            total = jnp.zeros((tokens // 2, chunk), jnp.float32)
            for half in range(2):
                total = total + jnp.dot(
                    side_of(hidden.at[half], side), down_own[half, :, columns],
                    preferred_element_type=jnp.float32,
                )
            store_part(MIXED, side, columns, total)

    def line_part(kind, which, number):
        if which:
            total = grad_line[0, kind, number].astype(jnp.float32)
            total = total + grad_line[2, kind, number].astype(jnp.float32)
        else:
            pair_at = (1 - pair, pair)[number]
            mine = pl.ds(pl.multiple_of((place * 2 + pair_at) * depth, depth), depth)
            total = grad_sum[kind, :, mine].astype(jnp.float32)
            total = total + grad_line[1, kind, number].astype(jnp.float32)
        return (total.T if kind == UP else total).astype(jnp.bfloat16)

    def blocks_at(kind, rep_at, pair_at):
        return grad_all.at[kind, pl.ds(block(rep_at, pair_at, 0), 2)]

    def grad_spread(kind, number):
        landed(grad_line.at[:, kind, number], gline_recv.at[kind, number], GRAD_LINE, kind, number)
        for which, low_at in enumerate((low, 1 - low)):
            if number:
                grad_all[kind, block(rep, pair, low_at)] = line_part(kind, which, number)
            else:
                grad_pair[kind, low_at] = line_part(kind, which, number)
        mine = blocks_at(kind, rep, pair)
        if number:
            go(mine, mine, grep_send.at[0], grep_recv.at[kind, 0], partner(X))
            grad_out(kind, rep, pair)
        else:
            go(grad_pair.at[kind], mine, gpair_send.at[0], gpair_recv.at[kind], partner(Y))

    def grad_pass(kind):
        near = blocks_at(kind, rep, 1 - pair)
        landed(near, gpair_recv.at[kind], GRAD_PAIR, kind)
        go(near, near, grep_send.at[0], grep_recv.at[kind, 1], partner(X))
        grad_out(kind, rep, 1 - pair)

    def store(source, target, number):
        pltpu.make_async_copy(source, target, store_sem.at[number]).start()

    def grad_out(kind, rep_at, pair_at):
        if (ROWS, kind) not in seen:
            seen.add((ROWS, kind))
            sums[kind].wait()
        for low_at in range(2):
            index = block(rep_at, pair_at, low_at)
            place_to = pl.ds(pl.multiple_of(index * own, own), own)
            if kind == UP:
                up_total[:, place_to] += grad_all[UP, index].astype(jnp.float32)
            else:
                down_total[place_to, :] += grad_all[DOWN, index].astype(jnp.float32)
        first = pl.ds(pl.multiple_of(block(rep_at, pair_at, 0) * own, own), 2 * own)
        at = (slice(None), first) if kind == UP else (first, slice(None))
        store((up_total, down_total)[kind].at[at], (up_out, down_out)[kind].at[at], kind)

    def grad_end(kind, number):
        pair_at = (pair, 1 - pair)[number]
        landed(blocks_at(kind, 1 - rep, pair_at), grep_recv.at[kind, number], GRAD_REP, kind, number)
        grad_out(kind, 1 - rep, pair_at)

    def share_rows(array):
        mine = rows_out.at[array, core]
        go(mine, mine, out_send.at[0], out_recv.at[array], other_core)
        store(mine, (input_out, mixed_out)[array].at[core], 2)

    def back_end():
        for side in range(2):
            scaled_rows = part_last(BACK, side) * gain
            at = pl.ds(side * (rows // 2), rows // 2)
            inverse, unit_rows, _ = norm_partial_terms(kept[at, :], gain)
            rows_out[BACK, core, side] = (
                inverse
                * (scaled_rows - unit_rows * jnp.mean(scaled_rows * unit_rows, axis=-1, keepdims=True))
            ).astype(jnp.bfloat16)
        share_rows(BACK)

    def mixed_end():
        for side in range(2):
            rows_out[MIXED, core, side] = part_last(MIXED, side).astype(jnp.bfloat16)
        share_rows(MIXED)

    def rows_end(array, out):
        landed(rows_out.at[array, 1 - core], out_recv.at[array], LAST, array)
        store(rows_out.at[array, 1 - core], out.at[1 - core], 2)

    def finish():
        for kind in KIND_ORDER:
            for number in range(2):
                grad_end(kind, number)
        rows_end(BACK, input_out)
        rows_end(MIXED, mixed_out)
        for number, whole in enumerate((up_total, down_total, rows_out)):
            pltpu.make_async_copy(whole, whole, store_sem.at[number]).wait()
        all_sent(tok.at[:, 1:], tok_send.at[0])
        all_sent(part.at[:, 1:], part_send.at[0])
        all_sent(up_own.at[:, : 3 * width // 4], line_send.at[0])
        all_sent(grad_sum.at[:, :, : 3 * width // 4], gline_send.at[0])
        all_sent(up_own.at[0, : width // 2], pair_send.at[0])
        all_sent(up_own, core_send.at[0])
        all_sent(grad_sent, share_send.at[0])
        all_sent(grad_pair, gpair_send.at[0])
        all_sent(grad_all.at[:, : n_fs // 2], grep_send.at[0])
        all_sent(rows_out.at[:, 0], out_send.at[0])

    sums = [
        pltpu.make_async_copy(up_sum_ref, up_total, sum_sem.at[UP]),
        pltpu.make_async_copy(down_sum_ref, down_total, sum_sem.at[DOWN]),
    ]
    for one in keep + sums:
        one.start()
    ends = (back_end, mixed_end)
    jobs = {
        TOK: send_tok, PAIR: pair_begin, LINE: line_begin, LINE_PASS: line_pass, CORE: to_core,
        PRE: saved_pre, GRAD: saved_grad, SHARE: grad_share, KEEP: grad_keep, GRAD_LINE: grad_begin, GRAD_GO: grad_go,
        GRAD_PAIR: grad_spread, GRAD_REP: grad_pass, BACK_SUMS: back_sums, MIXED_SUMS: mixed_sums,
        FIRST: part_first, SECOND: part_second, THIRD: part_third, LAST: lambda array: ends[array](),
        END: finish,
    }
    for job, *details in SCHEDULE:
        jobs[job](*details)


def store_kernel(*refs):
    count = len(refs) // 2
    copies = [
        pltpu.make_async_copy(refs[index], refs[count + index], refs[-1].at[index])
        for index in range(count)
    ]
    for one in copies:
        one.start()
    for one in copies:
        one.wait()


def cube_body(
    x_later, kept_input_rows, cotangent, norm_gain_vector, up_weight, down_weight, up_sum, down_sum
):
    row_count, width = x_later.shape
    n_fs = lax.axis_size("fs")
    grad_scale = float(row_count * lax.axis_size("rep") * n_fs) ** (-0.5)
    depth, units = up_weight.shape
    own = units // n_fs
    rows = row_count // 2
    outer = n_fs // 2
    tokens = n_fs * rows
    kind = x_later.dtype
    dma = pltpu.SemaphoreType.DMA
    vmem = functools.partial(pltpu.VMEM, dtype=kind)
    outside = pl.BlockSpec(memory_space=pltpu.HBM)
    results = pl.pallas_call(
        functools.partial(layer_kernel, n_fs, grad_scale),
        out_shape=(
            jax.ShapeDtypeStruct((2, 2, rows // 2, width), kind),
            jax.ShapeDtypeStruct((2, 2, rows // 2, width), kind),
            jax.ShapeDtypeStruct((depth, units), jnp.float32),
            jax.ShapeDtypeStruct((units, depth), jnp.float32),
        ),
        in_specs=[outside] * 8,
        out_specs=[pl.BlockSpec(memory_space=pl.ANY)] * 4,
        scratch_shapes=[
            pltpu.VMEM((1, width), jnp.float32), vmem((rows, width)), vmem((rows, width)), vmem((3, n_fs, 2, rows // 2, width)),
            vmem((2, width, own)), vmem((2, own, width)), vmem((depth, own)), vmem((own, depth)),
            pltpu.VMEM((2, tokens, own), jnp.float32), vmem((2, n_fs, 2, rows // 2, own)), vmem((2, n_fs, 2, rows // 2, own)),
            pltpu.VMEM((2, own, width), jnp.float32),
            vmem((2, own, width)), vmem((2, own, width)), vmem((2, own, width)),
            vmem((3, 2, 2, own, depth)), vmem((2, 2, own, depth)), vmem((2, n_fs, own, depth)),
            vmem((2, n_fs, 2, rows // 2, width)),
            vmem((2, 2, 4, rows // 2, width)), vmem((2, 2, 2, rows // 2, width)),
            vmem((2, 2, rows // 2, width)), vmem((2, 2, 2, rows // 2, width)),
            pltpu.VMEM((depth, units), jnp.float32), pltpu.VMEM((units, depth), jnp.float32),
            dma((5,)), dma((1,)), dma((2,)), dma((1,)), dma((3, 2)), dma((1,)), dma((2,)), dma((2,)),
            dma((1,)), dma((3, 2, 3)), dma((3, 2)), dma((1,)), dma((2,)), dma((1,)), dma((2, 2)),
            dma((1,)), dma((2,)), dma((1,)), dma((2, 2)), dma((1,)), dma((2, 2, 3)), dma((2,)),
            dma((1,)), dma((2,)), dma((2,)), dma((3,)),
        ],
        compiler_params=pltpu.CompilerParams(
            collective_id=0, has_side_effects=True, vmem_limit_bytes=VMEM_BYTES
        ),
    )(
        *[
            pltpu.with_memory_space_constraint(values, pltpu.HBM)
            for values in (
                x_later, kept_input_rows, cotangent, norm_gain_vector.reshape(1, width),
                up_weight, down_weight, up_sum, down_sum,
            )
        ],
    )
    results = [one.reshape(row_count, width) for one in results[:2]] + list(results[2:])
    return pl.pallas_call(
        store_kernel,
        out_shape=[jax.ShapeDtypeStruct(one.shape, one.dtype) for one in results],
        in_specs=[pl.BlockSpec(memory_space=pl.ANY)] * len(results),
        out_specs=[pl.BlockSpec(memory_space=pl.ANY)] * len(results),
        scratch_shapes=[dma((len(results),))],
        compiler_params=pltpu.CompilerParams(vmem_limit_bytes=2**20),
    )(*results)


def chosen_body(*args):
    depth, units = args[4].shape
    n_fs = lax.axis_size("fs")
    cubes = lax.axis_size("tp") == 2 and lax.axis_size("rep") == 2 and n_fs == 8
    return (cube_body if cubes and units == depth * n_fs and depth % 128 == 0 else body)(*args)


def solution(mesh):
    return jax.shard_map(
        chosen_body,
        mesh=mesh,
        in_specs=(
            P(("rep", "fs"), None),
            P(("rep", "fs"), None),
            P(("rep", "fs"), None),
            P(),
            P("fs", "tp"),
            P("tp", "fs"),
            P("fs", "tp"),
            P("tp", "fs"),
        ),
        out_specs=(P(("rep", "fs"), None), P(("rep", "fs"), None), P("fs", "tp"), P("tp", "fs")),
        check_vma=False,
    )
```

```python
import functools

import jax
import jax.numpy as jnp
from jax import lax
from jax.experimental import pallas as pl
from jax.experimental.pallas import tpu as pltpu
from jax.sharding import PartitionSpec as P

EPSILON = 1e-06
MESH = pl.DeviceIdType.MESH
TRANSPOSED = (((1,), (1,)), ((), ()))
LEADING = (((0,), (0,)), ((), ()))
X, Y, Z = 4, 2, 1
COT, SAVED, LATER = 0, 1, 2
BACK, MIXED = 0, 1
UP, DOWN = 0, 1
(TOK, PAIR, LINE, LINE_PASS, CORE, PRE, GRAD, SHARE, KEEP, GRAD_LINE,
 GRAD_PAIR, GRAD_REP, BACK_SUMS, MIXED_SUMS, FIRST, SECOND, THIRD, LAST, END, GRAD_GO, TOKENS, OWN, PARTS, ROWS) = range(24)
KIND_ORDER = (DOWN, UP)
TOKEN_ORDERS = (((Z, Y, X), (Z, X, Y)), ((Z, Y, X), (Z, Y, X)), ((Z, Y, X), (Z, X, Y)))
SUM_ORDERS = (((Y, X, Z), (X, Z, Y)), ((Y, X, Z), (Y, Z, X)))
SCHEDULE = (
    (TOK, COT, 0, 2), (TOK, SAVED, 1, 1), (TOK, COT, 1, 1), (TOK, COT, 0, 1), (TOK, SAVED, 1, 2),
    (LINE, DOWN, 2), (PAIR, UP), (TOK, COT, 1, 0), (PAIR, DOWN), (TOK, SAVED, 1, 5),
    (TOK, LATER, 1, 1), (TOK, SAVED, 0, 0), (TOK, COT, 1, 5), (LINE, UP, 2), (TOK, COT, 1, 3),
    (TOK, SAVED, 0, 1), (TOK, LATER, 1, 2), (TOK, SAVED, 1, 0), (LINE_PASS, UP, 3),
    (TOK, COT, 0, 0), (TOK, COT, 0, 5), (TOK, SAVED, 0, 4), (TOK, SAVED, 1, 3), (TOK, SAVED, 1, 4),
    (TOK, COT, 1, 6), (TOK, SAVED, 0, 3), (LINE, UP, 1), (LINE_PASS, UP, 2), (CORE, DOWN, 0),
    (LINE_PASS, UP, 1), (TOK, SAVED, 0, 2), (LINE_PASS, DOWN, 2), (TOK, LATER, 1, 0),
    (TOK, SAVED, 1, 6), (LINE, UP, 3), (TOK, COT, 0, 4), (TOK, COT, 0, 3), (TOK, COT, 1, 2),
    (TOK, LATER, 0, 0), (TOK, SAVED, 0, 5), (TOK, SAVED, 0, 6), (TOK, COT, 1, 4), (TOK, COT, 0, 6),
    (TOK, LATER, 1, 5), (LINE_PASS, DOWN, 1), (CORE, UP, 2), (LINE, DOWN, 3), (TOK, LATER, 1, 3),
    (TOK, LATER, 0, 3), (CORE, UP, 0), (CORE, UP, 3), (TOK, LATER, 0, 1), (TOK, LATER, 1, 4),
    (CORE, UP, 1), (PRE, 0), (LINE, DOWN, 1), (CORE, DOWN, 2), (LINE_PASS, DOWN, 3), (PRE, 1),
    (SHARE, DOWN), (TOK, LATER, 0, 4), (KEEP, DOWN), (TOK, LATER, 0, 2), (GRAD_LINE, DOWN),
    (GRAD_GO, DOWN, 0, 2), (TOK, LATER, 0, 6), (GRAD_GO, DOWN, 0, 1), (CORE, DOWN, 1),
    (GRAD_GO, DOWN, 0, 3), (TOK, LATER, 1, 6), (CORE, DOWN, 3), (GRAD_GO, DOWN, 1, 1), (GRAD, 0),
    (TOK, LATER, 0, 5), (GRAD, 1), (BACK_SUMS, 0), (FIRST, BACK, 0, 0), (BACK_SUMS, 1),
    (FIRST, BACK, 1, 1), (MIXED_SUMS, 1), (FIRST, MIXED, 1, 0), (GRAD_GO, DOWN, 1, 2),
    (FIRST, BACK, 1, 0), (MIXED_SUMS, 0), (SHARE, UP), (KEEP, UP), (GRAD_LINE, UP),
    (GRAD_GO, UP, 0, 1), (SECOND, MIXED, 1, 0), (FIRST, MIXED, 0, 0), (GRAD_GO, UP, 0, 3),
    (GRAD_GO, UP, 1, 1), (GRAD_PAIR, DOWN, 0), (GRAD_GO, UP, 0, 2), (SECOND, BACK, 0, 0),
    (SECOND, BACK, 0, 1), (GRAD_GO, DOWN, 1, 3), (SECOND, MIXED, 0, 0), (FIRST, MIXED, 1, 1),
    (SECOND, MIXED, 0, 1), (GRAD_REP, DOWN), (GRAD_PAIR, UP, 0), (GRAD_GO, UP, 1, 3),
    (SECOND, BACK, 1, 0), (FIRST, MIXED, 0, 1), (THIRD, MIXED, 1), (GRAD_PAIR, DOWN, 1),
    (SECOND, BACK, 1, 1), (GRAD_GO, UP, 1, 2), (GRAD_REP, UP), (SECOND, MIXED, 1, 1),
    (THIRD, MIXED, 0), (FIRST, BACK, 0, 1), (GRAD_PAIR, UP, 1), (THIRD, BACK, 1), (THIRD, BACK, 0),
    (LAST, MIXED), (LAST, BACK), (END,),
)
VMEM_BYTES = 48 * 2**20


def norm_partial_terms(values, norm_gain_vector):
    floats = values.astype(jnp.float32)
    inverse = lax.rsqrt(jnp.mean(floats * floats, axis=-1, keepdims=True) + EPSILON)
    unit_rows = floats * inverse
    normed = (unit_rows * norm_gain_vector).astype(jnp.bfloat16)
    return (inverse, unit_rows, normed)


def squared_relu(pre_act):
    return jnp.square(jax.nn.relu(pre_act)).astype(jnp.bfloat16)


def body(
    x_later, kept_input_rows, cotangent, norm_gain_vector, up_weight, down_weight, up_sum, down_sum
):
    row_count = x_later.shape[0]
    grad_scale = float(row_count * lax.axis_size("rep") * lax.axis_size("fs")) ** (-0.5)
    inv_later, unit_later, normed_later = norm_partial_terms(x_later, norm_gain_vector)
    inverse_rms_kept, unit_kept_rows, normed_kept_rows = norm_partial_terms(
        kept_input_rows, norm_gain_vector
    )
    stacked = jnp.concatenate([normed_kept_rows, normed_later], axis=0)
    up_whole = lax.all_gather(up_weight, "fs", axis=0, tiled=True)
    down_whole = lax.all_gather(down_weight, "fs", axis=1, tiled=True)
    pre_act = jnp.dot(stacked, up_whole, preferred_element_type=jnp.float32)
    pre_saved = pre_act[:row_count]
    hidden_saved = squared_relu(pre_saved)
    hidden_later = squared_relu(pre_act[row_count:])
    mixed_part = jnp.dot(hidden_later, down_whole, preferred_element_type=jnp.float32)
    hidden_grad = lax.dot_general(
        cotangent, down_whole, TRANSPOSED, preferred_element_type=jnp.float32
    )
    pre_grad = (hidden_grad * 2.0 * jax.nn.relu(pre_saved)).astype(jnp.bfloat16)
    back_part = lax.dot_general(pre_grad, up_whole, TRANSPOSED, preferred_element_type=jnp.float32)
    mixed_sum, back_sum = (
        lax.psum(mixed_part.astype(jnp.bfloat16), "tp").astype(jnp.float32),
        lax.psum(back_part.astype(jnp.bfloat16), "tp").astype(jnp.float32),
    )
    mixed = mixed_sum.astype(jnp.bfloat16)
    scaled_rows = back_sum * norm_gain_vector
    input_gradient_rows = (
        inverse_rms_kept
        * (
            scaled_rows
            - unit_kept_rows * jnp.mean(scaled_rows * unit_kept_rows, axis=-1, keepdims=True)
        )
    ).astype(jnp.bfloat16)
    cot_columns, normed_columns = (
        lax.all_to_all(cotangent, "fs", split_axis=1, concat_axis=0, tiled=True),
        lax.all_to_all(normed_kept_rows, "fs", split_axis=1, concat_axis=0, tiled=True),
    )
    columns = normed_columns
    up_grad = grad_scale * lax.dot_general(
        columns,
        lax.all_gather(pre_grad, "fs", axis=0, tiled=True),
        LEADING,
        preferred_element_type=jnp.float32,
    )
    columns = cot_columns
    down_grad = lax.dot_general(
        lax.all_gather(hidden_saved, "fs", axis=0, tiled=True),
        columns,
        LEADING,
        preferred_element_type=jnp.float32,
    )
    up_added, down_added = (
        lax.psum(up_grad.astype(jnp.bfloat16), "rep").astype(jnp.float32),
        lax.psum((down_grad * grad_scale).astype(jnp.bfloat16), "rep").astype(jnp.float32),
    )
    return (mixed, input_gradient_rows, up_sum + up_added, down_sum + down_added)

def layer_kernel(
    n_fs, grad_scale, x_ref, kept_ref, cot_ref, gain_ref, up_ref, down_ref, up_sum_ref, down_sum_ref,
    mixed_out, input_out, up_out, down_out,
    gain_kept, kept, fresh, tok, up_own, down_own, up_pass, down_pass, pre_kept, hidden, pre_grad,
    grad_kept, grad_sent, grad_got, grad_sum, grad_line, grad_pair, grad_all,
    part, got_first, got_second, got_third, rows_out, up_total, down_total,
    load_sem, pair_send, pair_recv, line_send, line_recv, core_send, core_recv, own_sem,
    tok_send, tok_recv, tok_last, share_send, share_recv, gline_send, gline_recv,
    gpair_send, gpair_recv, grep_send, grep_recv, part_send, part_recv, part_end,
    out_send, out_recv, sum_sem, store_sem,
):
    rep, fs, core = lax.axis_index("rep"), lax.axis_index("fs"), lax.axis_index("tp")
    outer = n_fs // 2
    place, pair = fs // 2, fs % 2
    low = place % 2
    half_rows, width = tok.shape[3:]
    rows = 2 * half_rows
    depth, own = up_pass.shape
    n_slots = tok.shape[1]
    tokens = n_slots * rows
    other_core = (rep, fs, 1 - core)
    start_row = pl.multiple_of(core * rows, rows)

    def place_at(step):
        return (place, place + 1 - 2 * low, (place + 2) % outer, outer - 1 - place)[step]

    def line_peer(step):
        return (rep, place_at(step) * 2 + pair, core)

    def partner(dim):
        if dim == X:
            return (1 - rep, fs, core)
        if dim == Y:
            return (rep, place * 2 + 1 - pair, core)
        return line_peer(1)

    def flip(bit, on):
        return 1 - bit if on else bit

    def slot(mask):
        return flip(rep, mask & X) * 4 + flip(pair, mask & Y) * 2 + flip(low, mask & Z)

    def block(rep_at, pair_at, low_at):
        return (rep_at * 2 + pair_at) * 2 + low_at

    def copy(source, target, send, recv, device):
        return pltpu.make_async_remote_copy(
            src_ref=source, dst_ref=target, send_sem=send, recv_sem=recv,
            device_id=device, device_id_type=MESH,
        )

    def reached(order, reach):
        return sum(dim for step, dim in enumerate(order) if reach >> step & 1)

    def go(source, target, send, recv, device):
        copy(source, target, send, recv, device).start()

    def all_sent(source, sem):
        copy(source, source, sem, sem, other_core).wait_send()

    seen = set()

    def landed(target, sem, *name):
        if name not in seen:
            seen.add(name)
            copy(target, target, sem, sem, other_core).wait_recv()

    own_rows = pl.ds(start_row, rows)

    def own_half(side):
        return pl.ds(pl.multiple_of(start_row + side * half_rows, half_rows), half_rows)

    loads = [
        pltpu.make_async_copy(kept_ref.at[own_rows, :], kept, load_sem.at[0]),
        pltpu.make_async_copy(x_ref.at[own_rows, :], fresh, load_sem.at[1]),
    ]
    loads += [
        pltpu.make_async_copy(
            cot_ref.at[own_half(side), :],
            tok.at[COT, slot(0), side], load_sem.at[2 + side],
        )
        for side in range(2)
    ]
    loads += [
        pltpu.make_async_copy(gain_ref, gain_kept, load_sem.at[4]),
    ]
    for one in loads:
        one.start()
    barrier = pltpu.get_barrier_semaphore()
    peers = [other_core, partner(X), partner(Y)] + [line_peer(step) for step in range(1, outer)]
    for peer in peers:
        pl.semaphore_signal(barrier, inc=1, device_id=peer, device_id_type=MESH)

    pl.semaphore_wait(barrier, len(peers))

    def own_ready(array):
        if (OWN, array, TOK) in seen:
            return
        seen.add((OWN, array, TOK))
        if array == COT:
            loads[2].wait()
            loads[3].wait()
            return
        if OWN not in seen:
            seen.add(OWN)
            loads[4].wait()
        loads[array == LATER].wait()
        normed = norm_partial_terms((kept if array == SAVED else fresh)[...], gain_kept[...])[2]
        tok[array, slot(0)] = normed.reshape(2, half_rows, width)

    def up_source(index):
        return up_ref.at[:, pl.ds(pl.multiple_of(index * own, own), own)]

    def down_source(index):
        return down_ref.at[pl.ds(pl.multiple_of(index * own, own), own), :]

    def up_slot(half, place_to, pair_to, count=1):
        first = pl.multiple_of((place_to * 2 + pair_to) * depth, depth)
        return up_own.at[half, pl.ds(first, count * depth), :]

    def down_slot(half, place_to, pair_to, count=1):
        first = pl.multiple_of((place_to * 2 + pair_to) * depth, depth)
        return down_own.at[half, :, pl.ds(first, count * depth)]

    def tok_landed(array, side, reach):
        mask = reached(TOKEN_ORDERS[array][side], reach)
        landed(tok.at[array, slot(mask), side], tok_recv.at[array, side, reach - 1], TOKENS, array, side, reach)

    def send_tok(array, side, number):
        reach, step = ((0, 0), (0, 1), (0, 2), (1, 1), (1, 2), (2, 2), (3, 2))[number]
        order = TOKEN_ORDERS[array][side]
        if reach:
            tok_landed(array, side, reach)
        at = tok.at[array, slot(reached(order, reach)), side]
        source = at
        if not reach and array == COT:
            source = cot_ref.at[own_half(side), :]
        elif not reach:
            own_ready(array)
        recv = tok_last.at[array, side] if step == 2 else tok_recv.at[array, side, (reach | 1 << step) - 1]
        go(source, at, tok_send.at[0], recv, partner(order[step]))

    def tok_end(array, which=(0, 1)):
        own_ready(array)
        for side in which:
            for reach in (1, 2, 3):
                tok_landed(array, side, reach)
            landed(tok.at[array, : n_slots // 2, side], tok_last.at[array, side], TOKENS, array, side)

    sides = (UP, DOWN)
    source_of = (up_source, down_source)
    slot_of = (up_slot, down_slot)
    pass_of = (up_pass, down_pass)

    def pair_begin(kind):
        for which, low_to in enumerate((low, 1 - low)):
            target = pass_of[kind] if which else slot_of[kind](core, place, pair)
            go(
                source_of[kind](block(rep, 1 - pair, low_to)), target,
                pair_send.at[0], pair_recv.at[kind], partner(Y),
            )

    def line_begin(kind, step):
        go(
            source_of[kind](block(rep, pair, flip(low, step % 2))), slot_of[kind](core, place, pair),
            line_send.at[0], line_recv.at[step - 1, kind], line_peer(step),
        )

    def pair_end(kind):
        landed(slot_of[kind](core, place, 0, 2), pair_recv.at[kind], PAIR, kind)

    def line_pass(kind, step):
        pair_end(kind)
        near = slot_of[kind](core, place, 1 - pair)
        go(
            pass_of[kind] if step % 2 else near, near,
            line_send.at[0], line_recv.at[step - 1, kind], line_peer(step),
        )

    def line_landed(kind, step):
        landed(slot_of[kind](core, place_at(step), 0, 2), line_recv.at[step - 1, kind], LINE, kind, step)

    def own_end(kind):
        pair_end(kind)
        if (OWN, kind) not in seen:
            seen.add((OWN, kind))
            keep[kind].wait()

    def to_core(kind, step):
        if step:
            line_landed(kind, step)
        else:
            own_end(kind)
        mine = slot_of[kind](core, place_at(step), 0, 2)
        go(mine, mine, core_send.at[0], core_recv.at[kind], other_core)

    def weights_end(kind, number):
        if number:
            landed((up_own, down_own)[kind].at[1 - core], core_recv.at[kind], CORE, kind)
        else:
            own_end(kind)
            for step in range(1, outer):
                line_landed(kind, step)

    keep = [
        pltpu.make_async_copy(
            source_of[kind](block(rep, pair, low)), slot_of[kind](core, place, pair), own_sem.at[kind]
        )
        for kind in sides
    ]

    def all_tokens(array):
        return tok[array].reshape(tokens, width)

    def saved_pre(number):
        half = (core, 1 - core)[number]
        tok_end(SAVED)
        weights_end(UP, number)
        pre = jnp.dot(all_tokens(SAVED), up_own[half], preferred_element_type=jnp.float32)
        pre_kept[half] = jax.nn.relu(pre)
        hidden[half] = squared_relu(pre).reshape(hidden.shape[1:])

    def saved_grad(number):
        half = (core, 1 - core)[number]
        tok_end(COT)
        weights_end(DOWN, number)
        grad = lax.dot_general(
            all_tokens(COT), down_own[half], TRANSPOSED, preferred_element_type=jnp.float32
        )
        pre_grad[half] = (grad * 2.0 * pre_kept[half]).astype(jnp.bfloat16).reshape(pre_grad.shape[1:])

    chunk = width // outer

    def chunk_at(index):
        return pl.ds(pl.multiple_of(index * chunk, chunk), chunk)

    def weight_grad(kind, half, columns):
        left = (hidden[half] if kind == DOWN else pre_grad[half]).reshape(tokens, own)
        right = tok[COT if kind == DOWN else SAVED, :, :, :, columns].reshape(tokens, chunk)
        return grad_scale * lax.dot_general(left, right, LEADING, preferred_element_type=jnp.float32)

    def grad_share(kind):
        if kind == DOWN:
            tok_end(COT)

        @pl.loop(0, outer)
        def _(index):
            columns = chunk_at(index)
            grad_sent[kind, :, columns] = weight_grad(kind, 1 - core, columns).astype(jnp.bfloat16)

        go(grad_sent.at[kind], grad_got.at[kind], share_send.at[0], share_recv.at[kind], other_core)

    def grad_keep(kind):
        if kind == DOWN:
            tok_end(COT)

        @pl.loop(0, outer)
        def _(index):
            columns = chunk_at(index)
            grad_kept[kind, :, columns] = weight_grad(kind, core, columns)

    def grad_begin(kind):
        landed(grad_got.at[kind], share_recv.at[kind], SHARE, kind)

        @pl.loop(0, outer)
        def _(index):
            columns = chunk_at(index)
            grad_sum[kind, :, columns] = (
                grad_kept[kind, :, columns] + grad_got[kind, :, columns].astype(jnp.float32)
            ).astype(jnp.bfloat16)

    def grad_go(kind, number, step):
        pair_at = (1 - pair, pair)[number]
        columns = pl.ds(pl.multiple_of((place_at(step) * 2 + pair_at) * depth, depth), depth)
        go(
            grad_sum.at[kind, :, columns], grad_line.at[step - 1, kind, number],
            gline_send.at[0], gline_recv.at[kind, number], line_peer(step),
        )

    def part_at(array, side, mask):
        return part.at[array, slot(mask), side]

    def part_mask(array, side, number):
        first, second, third = SUM_ORDERS[array][side]
        return (second | third, second, third, 0, third, 0)[number]

    def part_first(array, side, number):
        first = SUM_ORDERS[array][side][0]
        for place_in in (2 * number, 2 * number + 1):
            go(
                part_at(array, side, first | part_mask(array, side, place_in)),
                got_first.at[array, side, place_in],
                part_send.at[0], part_sem(array, side, place_in), partner(first),
            )

    def part_sem(array, side, number):
        if number in (3, 5, 6):
            return part_end.at[array]
        return part_recv.at[array, side, min(number, 2)]

    def part_add(array, side, mask, *got):
        total = part_at(array, side, mask)[...].astype(jnp.float32)
        for one in got:
            total = total + one[...].astype(jnp.float32)
        return total

    def part_second(array, side, number):
        mask = part_mask(array, side, number)
        got = got_first.at[array, side, number]
        landed(got, part_sem(array, side, number), SECOND, array, side, number)
        at = part_at(array, side, mask)
        at[...] = part_add(array, side, mask, got).astype(jnp.bfloat16)
        go(
            at, got_second.at[array, side, number],
            part_send.at[0], part_sem(array, side, 4 + number), partner(SUM_ORDERS[array][side][1]),
        )

    def part_third(array, side):
        third = SUM_ORDERS[array][side][2]
        got = (got_first.at[array, side, 2], got_second.at[array, side, 0])
        landed(got_second.at[array, side], part_sem(array, side, 2), THIRD, array, side)
        at = part_at(array, side, third)
        at[...] = part_add(array, side, third, *got).astype(jnp.bfloat16)
        go(
            at, got_third.at[array, side],
            part_send.at[0], part_sem(array, side, 6), partner(third),
        )

    def part_last(array, side):
        landed(part.at[array, : n_slots // 2 - 1], part_end.at[array], LAST, array, PARTS)
        return part_add(
            array, side, 0,
            got_first.at[array, side, 3], got_second.at[array, side, 1], got_third.at[array, side],
        )

    def side_of(ref, side):
        return ref[:, side].reshape(tokens // 2, ref.shape[-1])

    def store_part(array, side, columns, total):
        part[array, :, side, :, columns] = total.astype(jnp.bfloat16).reshape(n_slots, half_rows, chunk)

    def back_sums(side):
        @pl.loop(0, outer)
        def _(index):
            columns = chunk_at(index)
            total = jnp.zeros((tokens // 2, chunk), jnp.float32)
            for half in range(2):
                total = total + lax.dot_general(
                    side_of(pre_grad.at[half], side), up_own[half, columns, :], TRANSPOSED,
                    preferred_element_type=jnp.float32,
                )
            store_part(BACK, side, columns, total)

    def mixed_sums(side):
        tok_end(LATER, (side,))

        @pl.loop(0, 2)
        def _(half):
            hidden[half, :, side] = squared_relu(
                jnp.dot(
                    side_of(tok.at[LATER], side), up_own[half], preferred_element_type=jnp.float32
                )
            ).reshape(n_slots, half_rows, own)

        @pl.loop(0, outer)
        def _(index):
            columns = chunk_at(index)
            total = jnp.zeros((tokens // 2, chunk), jnp.float32)
            for half in range(2):
                total = total + jnp.dot(
                    side_of(hidden.at[half], side), down_own[half, :, columns],
                    preferred_element_type=jnp.float32,
                )
            store_part(MIXED, side, columns, total)

    def line_part(kind, which, number):
        if which:
            total = grad_line[0, kind, number].astype(jnp.float32)
            total = total + grad_line[2, kind, number].astype(jnp.float32)
        else:
            pair_at = (1 - pair, pair)[number]
            mine = pl.ds(pl.multiple_of((place * 2 + pair_at) * depth, depth), depth)
            total = grad_sum[kind, :, mine].astype(jnp.float32)
            total = total + grad_line[1, kind, number].astype(jnp.float32)
        return (total.T if kind == UP else total).astype(jnp.bfloat16)

    def blocks_at(kind, rep_at, pair_at):
        return grad_all.at[kind, pl.ds(block(rep_at, pair_at, 0), 2)]

    def grad_spread(kind, number):
        landed(grad_line.at[:, kind, number], gline_recv.at[kind, number], GRAD_LINE, kind, number)
        for which, low_at in enumerate((low, 1 - low)):
            if number:
                grad_all[kind, block(rep, pair, low_at)] = line_part(kind, which, number)
            else:
                grad_pair[kind, low_at] = line_part(kind, which, number)
        mine = blocks_at(kind, rep, pair)
        if number:
            go(mine, mine, grep_send.at[0], grep_recv.at[kind, 0], partner(X))
            grad_out(kind, rep, pair)
        else:
            go(grad_pair.at[kind], mine, gpair_send.at[0], gpair_recv.at[kind], partner(Y))

    def grad_pass(kind):
        near = blocks_at(kind, rep, 1 - pair)
        landed(near, gpair_recv.at[kind], GRAD_PAIR, kind)
        go(near, near, grep_send.at[0], grep_recv.at[kind, 1], partner(X))
        grad_out(kind, rep, 1 - pair)

    def store(source, target, number):
        pltpu.make_async_copy(source, target, store_sem.at[number]).start()

    def grad_out(kind, rep_at, pair_at):
        if (ROWS, kind) not in seen:
            seen.add((ROWS, kind))
            sums[kind].wait()
        for low_at in range(2):
            index = block(rep_at, pair_at, low_at)
            place_to = pl.ds(pl.multiple_of(index * own, own), own)
            if kind == UP:
                up_total[:, place_to] += grad_all[UP, index].astype(jnp.float32)
            else:
                down_total[place_to, :] += grad_all[DOWN, index].astype(jnp.float32)
        first = pl.ds(pl.multiple_of(block(rep_at, pair_at, 0) * own, own), 2 * own)
        at = (slice(None), first) if kind == UP else (first, slice(None))
        store((up_total, down_total)[kind].at[at], (up_out, down_out)[kind].at[at], kind)

    def grad_end(kind, number):
        pair_at = (pair, 1 - pair)[number]
        landed(blocks_at(kind, 1 - rep, pair_at), grep_recv.at[kind, number], GRAD_REP, kind, number)
        grad_out(kind, 1 - rep, pair_at)

    def share_rows(array):
        mine = rows_out.at[array, core]
        go(mine, mine, out_send.at[0], out_recv.at[array], other_core)
        store(mine, (input_out, mixed_out)[array].at[core], 2)

    def back_end():
        for side in range(2):
            scaled_rows = part_last(BACK, side) * gain_kept[...]
            at = pl.ds(side * (rows // 2), rows // 2)
            inverse, unit_rows, _ = norm_partial_terms(kept[at, :], gain_kept[...])
            rows_out[BACK, core, side] = (
                inverse
                * (scaled_rows - unit_rows * jnp.mean(scaled_rows * unit_rows, axis=-1, keepdims=True))
            ).astype(jnp.bfloat16)
        share_rows(BACK)

    def mixed_end():
        for side in range(2):
            rows_out[MIXED, core, side] = part_last(MIXED, side).astype(jnp.bfloat16)
        share_rows(MIXED)

    def rows_end(array, out):
        landed(rows_out.at[array, 1 - core], out_recv.at[array], LAST, array)
        store(rows_out.at[array, 1 - core], out.at[1 - core], 2)

    def finish():
        for kind in KIND_ORDER:
            for number in range(2):
                grad_end(kind, number)
        rows_end(BACK, input_out)
        rows_end(MIXED, mixed_out)
        for number, whole in enumerate((up_total, down_total, rows_out)):
            pltpu.make_async_copy(whole, whole, store_sem.at[number]).wait()
        all_sent(tok.at[:, 1:], tok_send.at[0])
        all_sent(part.at[:, 1:], part_send.at[0])
        all_sent(up_own.at[:, : 3 * width // 4], line_send.at[0])
        all_sent(grad_sum.at[:, :, : 3 * width // 4], gline_send.at[0])
        all_sent(up_own.at[0, : width // 2], pair_send.at[0])
        all_sent(up_own, core_send.at[0])
        all_sent(grad_sent, share_send.at[0])
        all_sent(grad_pair, gpair_send.at[0])
        all_sent(grad_all.at[:, : n_fs // 2], grep_send.at[0])
        all_sent(rows_out.at[:, 0], out_send.at[0])

    sums = [
        pltpu.make_async_copy(up_sum_ref, up_total, sum_sem.at[UP]),
        pltpu.make_async_copy(down_sum_ref, down_total, sum_sem.at[DOWN]),
    ]
    for one in keep + sums:
        one.start()
    ends = (back_end, mixed_end)
    jobs = {
        TOK: send_tok, PAIR: pair_begin, LINE: line_begin, LINE_PASS: line_pass, CORE: to_core,
        PRE: saved_pre, GRAD: saved_grad, SHARE: grad_share, KEEP: grad_keep, GRAD_LINE: grad_begin, GRAD_GO: grad_go,
        GRAD_PAIR: grad_spread, GRAD_REP: grad_pass, BACK_SUMS: back_sums, MIXED_SUMS: mixed_sums,
        FIRST: part_first, SECOND: part_second, THIRD: part_third, LAST: lambda array: ends[array](),
        END: finish,
    }
    for job, *details in SCHEDULE:
        jobs[job](*details)


def store_kernel(*refs):
    count = len(refs) // 2
    copies = [
        pltpu.make_async_copy(refs[index], refs[count + index], refs[-1].at[index])
        for index in range(count)
    ]
    for one in copies:
        one.start()
    for one in copies:
        one.wait()


def cube_body(
    x_later, kept_input_rows, cotangent, norm_gain_vector, up_weight, down_weight, up_sum, down_sum
):
    row_count, width = x_later.shape
    n_fs = lax.axis_size("fs")
    grad_scale = float(row_count * lax.axis_size("rep") * n_fs) ** (-0.5)
    depth, units = up_weight.shape
    own = units // n_fs
    rows = row_count // 2
    outer = n_fs // 2
    tokens = n_fs * rows
    kind = x_later.dtype
    dma = pltpu.SemaphoreType.DMA
    vmem = functools.partial(pltpu.VMEM, dtype=kind)
    outside = pl.BlockSpec(memory_space=pltpu.HBM)
    results = pl.pallas_call(
        functools.partial(layer_kernel, n_fs, grad_scale),
        out_shape=(
            jax.ShapeDtypeStruct((2, 2, rows // 2, width), kind),
            jax.ShapeDtypeStruct((2, 2, rows // 2, width), kind),
            jax.ShapeDtypeStruct((depth, units), jnp.float32),
            jax.ShapeDtypeStruct((units, depth), jnp.float32),
        ),
        in_specs=[outside] * 8,
        out_specs=[pl.BlockSpec(memory_space=pl.ANY)] * 4,
        scratch_shapes=[
            pltpu.VMEM((1, width), jnp.float32), vmem((rows, width)), vmem((rows, width)), vmem((3, n_fs, 2, rows // 2, width)),
            vmem((2, width, own)), vmem((2, own, width)), vmem((depth, own)), vmem((own, depth)),
            pltpu.VMEM((2, tokens, own), jnp.float32), vmem((2, n_fs, 2, rows // 2, own)), vmem((2, n_fs, 2, rows // 2, own)),
            pltpu.VMEM((2, own, width), jnp.float32),
            vmem((2, own, width)), vmem((2, own, width)), vmem((2, own, width)),
            vmem((3, 2, 2, own, depth)), vmem((2, 2, own, depth)), vmem((2, n_fs, own, depth)),
            vmem((2, n_fs, 2, rows // 2, width)),
            vmem((2, 2, 4, rows // 2, width)), vmem((2, 2, 2, rows // 2, width)),
            vmem((2, 2, rows // 2, width)), vmem((2, 2, 2, rows // 2, width)),
            pltpu.VMEM((depth, units), jnp.float32), pltpu.VMEM((units, depth), jnp.float32),
            dma((5,)), dma((1,)), dma((2,)), dma((1,)), dma((3, 2)), dma((1,)), dma((2,)), dma((2,)),
            dma((1,)), dma((3, 2, 3)), dma((3, 2)), dma((1,)), dma((2,)), dma((1,)), dma((2, 2)),
            dma((1,)), dma((2,)), dma((1,)), dma((2, 2)), dma((1,)), dma((2, 2, 3)), dma((2,)),
            dma((1,)), dma((2,)), dma((2,)), dma((3,)),
        ],
        compiler_params=pltpu.CompilerParams(
            collective_id=0, has_side_effects=True, vmem_limit_bytes=VMEM_BYTES
        ),
    )(
        *[
            pltpu.with_memory_space_constraint(values, pltpu.HBM)
            for values in (
                x_later, kept_input_rows, cotangent, norm_gain_vector.reshape(1, width),
                up_weight, down_weight, up_sum, down_sum,
            )
        ],
    )
    results = [one.reshape(row_count, width) for one in results[:2]] + list(results[2:])
    return pl.pallas_call(
        store_kernel,
        out_shape=[jax.ShapeDtypeStruct(one.shape, one.dtype) for one in results],
        in_specs=[pl.BlockSpec(memory_space=pl.ANY)] * len(results),
        out_specs=[pl.BlockSpec(memory_space=pl.ANY)] * len(results),
        scratch_shapes=[dma((len(results),))],
        compiler_params=pltpu.CompilerParams(vmem_limit_bytes=2**20),
    )(*results)


def chosen_body(*args):
    depth, units = args[4].shape
    n_fs = lax.axis_size("fs")
    cubes = lax.axis_size("tp") == 2 and lax.axis_size("rep") == 2 and n_fs == 8
    return (cube_body if cubes and units == depth * n_fs and depth % 128 == 0 else body)(*args)


def solution(mesh):
    return jax.shard_map(
        chosen_body,
        mesh=mesh,
        in_specs=(
            P(("rep", "fs"), None),
            P(("rep", "fs"), None),
            P(("rep", "fs"), None),
            P(),
            P("fs", "tp"),
            P("tp", "fs"),
            P("fs", "tp"),
            P("tp", "fs"),
        ),
        out_specs=(P(("rep", "fs"), None), P(("rep", "fs"), None), P("fs", "tp"), P("tp", "fs")),
        check_vma=False,
    )
```

```python
import functools

import jax
import jax.numpy as jnp
from jax import lax
from jax.experimental import pallas as pl
from jax.experimental.pallas import tpu as pltpu
from jax.sharding import PartitionSpec as P

EPSILON = 1e-06
MESH = pl.DeviceIdType.MESH
TRANSPOSED = (((1,), (1,)), ((), ()))
LEADING = (((0,), (0,)), ((), ()))
X, Y, Z = 4, 2, 1
COT, SAVED, LATER = 0, 1, 2
BACK, MIXED = 0, 1
UP, DOWN = 0, 1
(TOK, PAIR, LINE, LINE_PASS, CORE, PRE, GRAD, SHARE, KEEP, GRAD_LINE,
 GRAD_PAIR, GRAD_REP, BACK_SUMS, MIXED_SUMS, FIRST, SECOND, THIRD, LAST, END, GRAD_GO, TOKENS, OWN, PARTS, ROWS) = range(24)
KIND_ORDER = (DOWN, UP)
TOKEN_ORDERS = (((Z, Y, X), (Z, X, Y)), ((Z, Y, X), (Z, Y, X)), ((Z, Y, X), (Z, X, Y)))
SUM_ORDERS = (((Y, X, Z), (X, Z, Y)), ((Y, X, Z), (Y, Z, X)))
SCHEDULE = (
    (TOK, COT, 0, 2), (TOK, SAVED, 1, 1), (TOK, COT, 1, 1), (TOK, COT, 0, 1), (TOK, SAVED, 1, 2),
    (LINE, DOWN, 2), (PAIR, UP), (TOK, COT, 1, 0), (PAIR, DOWN), (TOK, SAVED, 1, 5),
    (TOK, LATER, 1, 1), (TOK, SAVED, 0, 0), (TOK, COT, 1, 5), (LINE, UP, 2), (TOK, COT, 1, 3),
    (TOK, SAVED, 0, 1), (TOK, LATER, 1, 2), (TOK, SAVED, 1, 0), (LINE_PASS, UP, 3),
    (TOK, COT, 0, 0), (TOK, COT, 0, 5), (TOK, SAVED, 0, 4), (TOK, SAVED, 1, 3), (TOK, SAVED, 1, 4),
    (TOK, COT, 1, 6), (TOK, SAVED, 0, 3), (LINE, UP, 1), (LINE_PASS, UP, 2), (CORE, DOWN, 0),
    (LINE_PASS, UP, 1), (TOK, SAVED, 0, 2), (LINE_PASS, DOWN, 2), (TOK, LATER, 1, 0),
    (TOK, SAVED, 1, 6), (LINE, UP, 3), (TOK, COT, 0, 4), (TOK, COT, 0, 3), (TOK, COT, 1, 2),
    (TOK, LATER, 0, 0), (TOK, SAVED, 0, 5), (TOK, SAVED, 0, 6), (TOK, COT, 1, 4), (TOK, COT, 0, 6),
    (TOK, LATER, 1, 5), (LINE_PASS, DOWN, 1), (CORE, UP, 2), (LINE, DOWN, 3), (TOK, LATER, 1, 3),
    (TOK, LATER, 0, 3), (CORE, UP, 0), (CORE, UP, 3), (TOK, LATER, 0, 1), (TOK, LATER, 1, 4),
    (CORE, UP, 1), (PRE, 0), (LINE, DOWN, 1), (CORE, DOWN, 2), (LINE_PASS, DOWN, 3), (PRE, 1),
    (SHARE, DOWN), (TOK, LATER, 0, 4), (KEEP, DOWN), (TOK, LATER, 0, 2), (GRAD_LINE, DOWN),
    (GRAD_GO, DOWN, 0, 2), (TOK, LATER, 0, 6), (GRAD_GO, DOWN, 0, 1), (CORE, DOWN, 1),
    (GRAD_GO, DOWN, 0, 3), (TOK, LATER, 1, 6), (CORE, DOWN, 3), (GRAD_GO, DOWN, 1, 1), (GRAD, 0),
    (TOK, LATER, 0, 5), (GRAD, 1), (BACK_SUMS, 0), (FIRST, BACK, 0, 0), (BACK_SUMS, 1),
    (FIRST, BACK, 1, 1), (MIXED_SUMS, 1), (FIRST, MIXED, 1, 0), (GRAD_GO, DOWN, 1, 2),
    (FIRST, BACK, 1, 0), (MIXED_SUMS, 0), (SHARE, UP), (KEEP, UP), (GRAD_LINE, UP),
    (GRAD_GO, UP, 0, 1), (SECOND, MIXED, 1, 0), (FIRST, MIXED, 0, 0), (GRAD_GO, UP, 0, 3),
    (GRAD_GO, UP, 1, 1), (GRAD_PAIR, DOWN, 0), (GRAD_GO, UP, 0, 2), (SECOND, BACK, 0, 0),
    (SECOND, BACK, 0, 1), (GRAD_GO, DOWN, 1, 3), (SECOND, MIXED, 0, 0), (FIRST, MIXED, 1, 1),
    (SECOND, MIXED, 0, 1), (GRAD_REP, DOWN), (GRAD_PAIR, UP, 0), (GRAD_GO, UP, 1, 3),
    (SECOND, BACK, 1, 0), (FIRST, MIXED, 0, 1), (THIRD, MIXED, 1), (GRAD_PAIR, DOWN, 1),
    (SECOND, BACK, 1, 1), (GRAD_GO, UP, 1, 2), (GRAD_REP, UP), (SECOND, MIXED, 1, 1),
    (THIRD, MIXED, 0), (FIRST, BACK, 0, 1), (GRAD_PAIR, UP, 1), (THIRD, BACK, 1), (THIRD, BACK, 0),
    (LAST, MIXED), (LAST, BACK), (END,),
)
VMEM_BYTES = 48 * 2**20


def norm_partial_terms(values, norm_gain_vector):
    floats = values.astype(jnp.float32)
    inverse = lax.rsqrt(jnp.mean(floats * floats, axis=-1, keepdims=True) + EPSILON)
    unit_rows = floats * inverse
    normed = (unit_rows * norm_gain_vector).astype(jnp.bfloat16)
    return (inverse, unit_rows, normed)


def squared_relu(pre_act):
    return jnp.square(jax.nn.relu(pre_act)).astype(jnp.bfloat16)


def body(
    x_later, kept_input_rows, cotangent, norm_gain_vector, up_weight, down_weight, up_sum, down_sum
):
    row_count = x_later.shape[0]
    grad_scale = float(row_count * lax.axis_size("rep") * lax.axis_size("fs")) ** (-0.5)
    inv_later, unit_later, normed_later = norm_partial_terms(x_later, norm_gain_vector)
    inverse_rms_kept, unit_kept_rows, normed_kept_rows = norm_partial_terms(
        kept_input_rows, norm_gain_vector
    )
    stacked = jnp.concatenate([normed_kept_rows, normed_later], axis=0)
    up_whole = lax.all_gather(up_weight, "fs", axis=0, tiled=True)
    down_whole = lax.all_gather(down_weight, "fs", axis=1, tiled=True)
    pre_act = jnp.dot(stacked, up_whole, preferred_element_type=jnp.float32)
    pre_saved = pre_act[:row_count]
    hidden_saved = squared_relu(pre_saved)
    hidden_later = squared_relu(pre_act[row_count:])
    mixed_part = jnp.dot(hidden_later, down_whole, preferred_element_type=jnp.float32)
    hidden_grad = lax.dot_general(
        cotangent, down_whole, TRANSPOSED, preferred_element_type=jnp.float32
    )
    pre_grad = (hidden_grad * 2.0 * jax.nn.relu(pre_saved)).astype(jnp.bfloat16)
    back_part = lax.dot_general(pre_grad, up_whole, TRANSPOSED, preferred_element_type=jnp.float32)
    mixed_sum, back_sum = (
        lax.psum(mixed_part.astype(jnp.bfloat16), "tp").astype(jnp.float32),
        lax.psum(back_part.astype(jnp.bfloat16), "tp").astype(jnp.float32),
    )
    mixed = mixed_sum.astype(jnp.bfloat16)
    scaled_rows = back_sum * norm_gain_vector
    input_gradient_rows = (
        inverse_rms_kept
        * (
            scaled_rows
            - unit_kept_rows * jnp.mean(scaled_rows * unit_kept_rows, axis=-1, keepdims=True)
        )
    ).astype(jnp.bfloat16)
    cot_columns, normed_columns = (
        lax.all_to_all(cotangent, "fs", split_axis=1, concat_axis=0, tiled=True),
        lax.all_to_all(normed_kept_rows, "fs", split_axis=1, concat_axis=0, tiled=True),
    )
    columns = normed_columns
    up_grad = grad_scale * lax.dot_general(
        columns,
        lax.all_gather(pre_grad, "fs", axis=0, tiled=True),
        LEADING,
        preferred_element_type=jnp.float32,
    )
    columns = cot_columns
    down_grad = lax.dot_general(
        lax.all_gather(hidden_saved, "fs", axis=0, tiled=True),
        columns,
        LEADING,
        preferred_element_type=jnp.float32,
    )
    up_added, down_added = (
        lax.psum(up_grad.astype(jnp.bfloat16), "rep").astype(jnp.float32),
        lax.psum((down_grad * grad_scale).astype(jnp.bfloat16), "rep").astype(jnp.float32),
    )
    return (mixed, input_gradient_rows, up_sum + up_added, down_sum + down_added)

def layer_kernel(
    n_fs, grad_scale, x_ref, kept_ref, cot_ref, gain_ref, up_ref, down_ref, up_sum_ref, down_sum_ref,
    mixed_out, input_out, up_out, down_out,
    gain_kept, kept, fresh, tok, up_own, down_own, up_pass, down_pass, pre_kept, hidden, pre_grad,
    grad_kept, grad_sent, grad_got, grad_sum, grad_line, grad_pair, grad_all,
    part, got_first, got_second, got_third, rows_out, up_total, down_total,
    load_sem, pair_send, pair_recv, line_send, line_recv, core_send, core_recv, own_sem,
    tok_send, tok_recv, tok_last, share_send, share_recv, gline_send, gline_recv,
    gpair_send, gpair_recv, grep_send, grep_recv, part_send, part_recv, part_end,
    out_send, out_recv, sum_sem, store_sem,
):
    rep, fs, core = lax.axis_index("rep"), lax.axis_index("fs"), lax.axis_index("tp")
    outer = n_fs // 2
    place, pair = fs // 2, fs % 2
    low = place % 2
    half_rows, width = tok.shape[3:]
    rows = 2 * half_rows
    depth, own = up_pass.shape
    n_slots = tok.shape[1]
    tokens = n_slots * rows
    other_core = (rep, fs, 1 - core)
    start_row = pl.multiple_of(core * rows, rows)

    def place_at(step):
        return (place, place + 1 - 2 * low, (place + 2) % outer, outer - 1 - place)[step]

    def line_peer(step):
        return (rep, place_at(step) * 2 + pair, core)

    def partner(dim):
        if dim == X:
            return (1 - rep, fs, core)
        if dim == Y:
            return (rep, place * 2 + 1 - pair, core)
        return line_peer(1)

    def flip(bit, on):
        return 1 - bit if on else bit

    def slot(mask):
        return flip(rep, mask & X) * 4 + flip(pair, mask & Y) * 2 + flip(low, mask & Z)

    def block(rep_at, pair_at, low_at):
        return (rep_at * 2 + pair_at) * 2 + low_at

    def copy(source, target, send, recv, device):
        return pltpu.make_async_remote_copy(
            src_ref=source, dst_ref=target, send_sem=send, recv_sem=recv,
            device_id=device, device_id_type=MESH,
        )

    def reached(order, reach):
        return sum(dim for step, dim in enumerate(order) if reach >> step & 1)

    def go(source, target, send, recv, device):
        copy(source, target, send, recv, device).start()

    def all_sent(source, sem):
        copy(source, source, sem, sem, other_core).wait_send()

    seen = set()

    def landed(target, sem, *name):
        if name not in seen:
            seen.add(name)
            copy(target, target, sem, sem, other_core).wait_recv()

    own_rows = pl.ds(start_row, rows)

    def own_half(side):
        return pl.ds(pl.multiple_of(start_row + side * half_rows, half_rows), half_rows)

    loads = [
        pltpu.make_async_copy(kept_ref.at[own_rows, :], kept, load_sem.at[0]),
        pltpu.make_async_copy(x_ref.at[own_rows, :], fresh, load_sem.at[1]),
    ]
    loads += [
        pltpu.make_async_copy(
            cot_ref.at[own_half(side), :],
            tok.at[COT, slot(0), side], load_sem.at[2 + side],
        )
        for side in range(2)
    ]
    loads += [
        pltpu.make_async_copy(gain_ref, gain_kept, load_sem.at[4]),
    ]
    for one in loads:
        one.start()
    barrier = pltpu.get_barrier_semaphore()
    peers = [other_core, partner(X), partner(Y)] + [line_peer(step) for step in range(1, outer)]
    for peer in peers:
        pl.semaphore_signal(barrier, inc=1, device_id=peer, device_id_type=MESH)

    pl.semaphore_wait(barrier, len(peers))

    def own_ready(array):
        if (OWN, array, TOK) in seen:
            return
        seen.add((OWN, array, TOK))
        if array == COT:
            loads[2].wait()
            loads[3].wait()
            return
        if OWN not in seen:
            seen.add(OWN)
            loads[4].wait()
        loads[array == LATER].wait()
        normed = norm_partial_terms((kept if array == SAVED else fresh)[...], gain_kept[...])[2]
        tok[array, slot(0)] = normed.reshape(2, half_rows, width)

    def up_source(index):
        return up_ref.at[:, pl.ds(pl.multiple_of(index * own, own), own)]

    def down_source(index):
        return down_ref.at[pl.ds(pl.multiple_of(index * own, own), own), :]

    def up_slot(half, place_to, pair_to, count=1):
        first = pl.multiple_of((place_to * 2 + pair_to) * depth, depth)
        return up_own.at[half, pl.ds(first, count * depth), :]

    def down_slot(half, place_to, pair_to, count=1):
        first = pl.multiple_of((place_to * 2 + pair_to) * depth, depth)
        return down_own.at[half, :, pl.ds(first, count * depth)]

    def tok_landed(array, side, reach):
        mask = reached(TOKEN_ORDERS[array][side], reach)
        landed(tok.at[array, slot(mask), side], tok_recv.at[array, side, reach - 1], TOKENS, array, side, reach)

    def send_tok(array, side, number):
        reach, step = ((0, 0), (0, 1), (0, 2), (1, 1), (1, 2), (2, 2), (3, 2))[number]
        order = TOKEN_ORDERS[array][side]
        if reach:
            tok_landed(array, side, reach)
        at = tok.at[array, slot(reached(order, reach)), side]
        source = at
        if not reach and array == COT:
            source = cot_ref.at[own_half(side), :]
        elif not reach:
            own_ready(array)
        recv = tok_last.at[array, side] if step == 2 else tok_recv.at[array, side, (reach | 1 << step) - 1]
        go(source, at, tok_send.at[0], recv, partner(order[step]))

    def tok_end(array, which=(0, 1)):
        own_ready(array)
        for side in which:
            for reach in (1, 2, 3):
                tok_landed(array, side, reach)
            landed(tok.at[array, : n_slots // 2, side], tok_last.at[array, side], TOKENS, array, side)

    sides = (UP, DOWN)
    source_of = (up_source, down_source)
    slot_of = (up_slot, down_slot)
    pass_of = (up_pass, down_pass)

    def pair_begin(kind):
        for which, low_to in enumerate((low, 1 - low)):
            target = pass_of[kind] if which else slot_of[kind](core, place, pair)
            go(
                source_of[kind](block(rep, 1 - pair, low_to)), target,
                pair_send.at[0], pair_recv.at[kind], partner(Y),
            )

    def line_begin(kind, step):
        go(
            source_of[kind](block(rep, pair, flip(low, step % 2))), slot_of[kind](core, place, pair),
            line_send.at[0], line_recv.at[step - 1, kind], line_peer(step),
        )

    def pair_end(kind):
        landed(slot_of[kind](core, place, 0, 2), pair_recv.at[kind], PAIR, kind)

    def line_pass(kind, step):
        pair_end(kind)
        near = slot_of[kind](core, place, 1 - pair)
        go(
            pass_of[kind] if step % 2 else near, near,
            line_send.at[0], line_recv.at[step - 1, kind], line_peer(step),
        )

    def line_landed(kind, step):
        landed(slot_of[kind](core, place_at(step), 0, 2), line_recv.at[step - 1, kind], LINE, kind, step)

    def own_end(kind):
        pair_end(kind)
        if (OWN, kind) not in seen:
            seen.add((OWN, kind))
            keep[kind].wait()

    def to_core(kind, step):
        if step:
            line_landed(kind, step)
        else:
            own_end(kind)
        mine = slot_of[kind](core, place_at(step), 0, 2)
        go(mine, mine, core_send.at[0], core_recv.at[kind], other_core)

    def weights_end(kind, number):
        if number:
            landed((up_own, down_own)[kind].at[1 - core], core_recv.at[kind], CORE, kind)
        else:
            own_end(kind)
            for step in range(1, outer):
                line_landed(kind, step)

    keep = [
        pltpu.make_async_copy(
            source_of[kind](block(rep, pair, low)), slot_of[kind](core, place, pair), own_sem.at[kind]
        )
        for kind in sides
    ]

    def all_tokens(array):
        return tok[array].reshape(tokens, width)

    def saved_pre(number):
        half = (core, 1 - core)[number]
        tok_end(SAVED)
        weights_end(UP, number)
        pre = jnp.dot(all_tokens(SAVED), up_own[half], preferred_element_type=jnp.float32)
        pre_kept[half] = jax.nn.relu(pre)
        hidden[half] = squared_relu(pre).reshape(hidden.shape[1:])

    def saved_grad(number):
        half = (core, 1 - core)[number]
        tok_end(COT)
        weights_end(DOWN, number)
        grad = lax.dot_general(
            all_tokens(COT), down_own[half], TRANSPOSED, preferred_element_type=jnp.float32
        )
        pre_grad[half] = (grad * 2.0 * pre_kept[half]).astype(jnp.bfloat16).reshape(pre_grad.shape[1:])

    chunk = width // outer

    def chunk_at(index):
        return pl.ds(pl.multiple_of(index * chunk, chunk), chunk)

    def weight_grad(kind, half, columns):
        left = (hidden[half] if kind == DOWN else pre_grad[half]).reshape(tokens, own)
        right = tok[COT if kind == DOWN else SAVED, :, :, :, columns].reshape(tokens, chunk)
        return grad_scale * lax.dot_general(left, right, LEADING, preferred_element_type=jnp.float32)

    def grad_share(kind):
        if kind == DOWN:
            tok_end(COT)

        @pl.loop(0, outer)
        def _(index):
            columns = chunk_at(index)
            grad_sent[kind, :, columns] = weight_grad(kind, 1 - core, columns).astype(jnp.bfloat16)

        go(grad_sent.at[kind], grad_got.at[kind], share_send.at[0], share_recv.at[kind], other_core)

    def grad_keep(kind):
        if kind == DOWN:
            tok_end(COT)

        @pl.loop(0, outer)
        def _(index):
            columns = chunk_at(index)
            grad_kept[kind, :, columns] = weight_grad(kind, core, columns)

    def grad_begin(kind):
        landed(grad_got.at[kind], share_recv.at[kind], SHARE, kind)

        @pl.loop(0, outer)
        def _(index):
            columns = chunk_at(index)
            grad_sum[kind, :, columns] = (
                grad_kept[kind, :, columns] + grad_got[kind, :, columns].astype(jnp.float32)
            ).astype(jnp.bfloat16)

    def grad_go(kind, number, step):
        pair_at = (1 - pair, pair)[number]
        columns = pl.ds(pl.multiple_of((place_at(step) * 2 + pair_at) * depth, depth), depth)
        go(
            grad_sum.at[kind, :, columns], grad_line.at[step - 1, kind, number],
            gline_send.at[0], gline_recv.at[kind, number], line_peer(step),
        )

    def part_at(array, side, mask):
        return part.at[array, slot(mask), side]

    def part_mask(array, side, number):
        first, second, third = SUM_ORDERS[array][side]
        return (second | third, second, third, 0, third, 0)[number]

    def part_first(array, side, number):
        first = SUM_ORDERS[array][side][0]
        for place_in in (2 * number, 2 * number + 1):
            go(
                part_at(array, side, first | part_mask(array, side, place_in)),
                got_first.at[array, side, place_in],
                part_send.at[0], part_sem(array, side, place_in), partner(first),
            )

    def part_sem(array, side, number):
        if number in (3, 5, 6):
            return part_end.at[array]
        return part_recv.at[array, side, min(number, 2)]

    def part_add(array, side, mask, *got):
        total = part_at(array, side, mask)[...].astype(jnp.float32)
        for one in got:
            total = total + one[...].astype(jnp.float32)
        return total

    def part_second(array, side, number):
        mask = part_mask(array, side, number)
        got = got_first.at[array, side, number]
        landed(got, part_sem(array, side, number), SECOND, array, side, number)
        at = part_at(array, side, mask)
        at[...] = part_add(array, side, mask, got).astype(jnp.bfloat16)
        go(
            at, got_second.at[array, side, number],
            part_send.at[0], part_sem(array, side, 4 + number), partner(SUM_ORDERS[array][side][1]),
        )

    def part_third(array, side):
        third = SUM_ORDERS[array][side][2]
        got = (got_first.at[array, side, 2], got_second.at[array, side, 0])
        landed(got_second.at[array, side], part_sem(array, side, 2), THIRD, array, side)
        at = part_at(array, side, third)
        at[...] = part_add(array, side, third, *got).astype(jnp.bfloat16)
        go(
            at, got_third.at[array, side],
            part_send.at[0], part_sem(array, side, 6), partner(third),
        )

    def part_last(array, side):
        landed(part.at[array, : n_slots // 2 - 1], part_end.at[array], LAST, array, PARTS)
        return part_add(
            array, side, 0,
            got_first.at[array, side, 3], got_second.at[array, side, 1], got_third.at[array, side],
        )

    def side_of(ref, side):
        return ref[:, side].reshape(tokens // 2, ref.shape[-1])

    def store_part(array, side, columns, total):
        part[array, :, side, :, columns] = total.astype(jnp.bfloat16).reshape(n_slots, half_rows, chunk)

    def back_sums(side):
        @pl.loop(0, outer)
        def _(index):
            columns = chunk_at(index)
            total = jnp.zeros((tokens // 2, chunk), jnp.float32)
            for half in range(2):
                total = total + lax.dot_general(
                    side_of(pre_grad.at[half], side), up_own[half, columns, :], TRANSPOSED,
                    preferred_element_type=jnp.float32,
                )
            store_part(BACK, side, columns, total)

    def mixed_sums(side):
        tok_end(LATER, (side,))

        @pl.loop(0, 2)
        def _(half):
            hidden[half, :, side] = squared_relu(
                jnp.dot(
                    side_of(tok.at[LATER], side), up_own[half], preferred_element_type=jnp.float32
                )
            ).reshape(n_slots, half_rows, own)

        @pl.loop(0, outer)
        def _(index):
            columns = chunk_at(index)
            total = jnp.zeros((tokens // 2, chunk), jnp.float32)
            for half in range(2):
                total = total + jnp.dot(
                    side_of(hidden.at[half], side), down_own[half, :, columns],
                    preferred_element_type=jnp.float32,
                )
            store_part(MIXED, side, columns, total)

    def line_part(kind, which, number):
        if which:
            total = grad_line[0, kind, number].astype(jnp.float32)
            total = total + grad_line[2, kind, number].astype(jnp.float32)
        else:
            pair_at = (1 - pair, pair)[number]
            mine = pl.ds(pl.multiple_of((place * 2 + pair_at) * depth, depth), depth)
            total = grad_sum[kind, :, mine].astype(jnp.float32)
            total = total + grad_line[1, kind, number].astype(jnp.float32)
        return (total.T if kind == UP else total).astype(jnp.bfloat16)

    def blocks_at(kind, rep_at, pair_at):
        return grad_all.at[kind, pl.ds(block(rep_at, pair_at, 0), 2)]

    def grad_spread(kind, number):
        landed(grad_line.at[:, kind, number], gline_recv.at[kind, number], GRAD_LINE, kind, number)
        for which, low_at in enumerate((low, 1 - low)):
            if number:
                grad_all[kind, block(rep, pair, low_at)] = line_part(kind, which, number)
            else:
                grad_pair[kind, low_at] = line_part(kind, which, number)
        mine = blocks_at(kind, rep, pair)
        if number:
            go(mine, mine, grep_send.at[0], grep_recv.at[kind, 0], partner(X))
            grad_out(kind, rep, pair)
        else:
            go(grad_pair.at[kind], mine, gpair_send.at[0], gpair_recv.at[kind], partner(Y))

    def grad_pass(kind):
        near = blocks_at(kind, rep, 1 - pair)
        landed(near, gpair_recv.at[kind], GRAD_PAIR, kind)
        go(near, near, grep_send.at[0], grep_recv.at[kind, 1], partner(X))
        grad_out(kind, rep, 1 - pair)

    def store(source, target, number):
        pltpu.make_async_copy(source, target, store_sem.at[number]).start()

    def grad_out(kind, rep_at, pair_at):
        if (ROWS, kind) not in seen:
            seen.add((ROWS, kind))
            sums[kind].wait()
        for low_at in range(2):
            index = block(rep_at, pair_at, low_at)
            place_to = pl.ds(pl.multiple_of(index * own, own), own)
            if kind == UP:
                up_total[:, place_to] += grad_all[UP, index].astype(jnp.float32)
            else:
                down_total[place_to, :] += grad_all[DOWN, index].astype(jnp.float32)
        first = pl.ds(pl.multiple_of(block(rep_at, pair_at, 0) * own, own), 2 * own)
        at = (slice(None), first) if kind == UP else (first, slice(None))
        store((up_total, down_total)[kind].at[at], (up_out, down_out)[kind].at[at], kind)

    def grad_end(kind, number):
        pair_at = (pair, 1 - pair)[number]
        landed(blocks_at(kind, 1 - rep, pair_at), grep_recv.at[kind, number], GRAD_REP, kind, number)
        grad_out(kind, 1 - rep, pair_at)

    def share_rows(array):
        mine = rows_out.at[array, core]
        go(mine, mine, out_send.at[0], out_recv.at[array], other_core)
        store(mine, (input_out, mixed_out)[array].at[core], 2)

    def back_end():
        for side in range(2):
            scaled_rows = part_last(BACK, side) * gain_kept[...]
            at = pl.ds(side * (rows // 2), rows // 2)
            inverse, unit_rows, _ = norm_partial_terms(kept[at, :], gain_kept[...])
            rows_out[BACK, core, side] = (
                inverse
                * (scaled_rows - unit_rows * jnp.mean(scaled_rows * unit_rows, axis=-1, keepdims=True))
            ).astype(jnp.bfloat16)
        share_rows(BACK)

    def mixed_end():
        for side in range(2):
            rows_out[MIXED, core, side] = part_last(MIXED, side).astype(jnp.bfloat16)
        share_rows(MIXED)

    def rows_end(array, out):
        landed(rows_out.at[array, 1 - core], out_recv.at[array], LAST, array)
        store(rows_out.at[array, 1 - core], out.at[1 - core], 2)

    def finish():
        first, last = KIND_ORDER
        grad_end(first, 0)
        grad_end(first, 1)
        grad_end(last, 1)
        rows_end(BACK, input_out)
        rows_end(MIXED, mixed_out)
        grad_end(last, 0)
        for number, whole in enumerate((up_total, down_total, rows_out)):
            pltpu.make_async_copy(whole, whole, store_sem.at[number]).wait()
        all_sent(tok.at[:, 1:], tok_send.at[0])
        all_sent(part.at[:, 1:], part_send.at[0])
        all_sent(up_own.at[:, : 3 * width // 4], line_send.at[0])
        all_sent(grad_sum.at[:, :, : 3 * width // 4], gline_send.at[0])
        all_sent(up_own.at[0, : width // 2], pair_send.at[0])
        all_sent(up_own, core_send.at[0])
        all_sent(grad_sent, share_send.at[0])
        all_sent(grad_pair, gpair_send.at[0])
        all_sent(grad_all.at[:, : n_fs // 2], grep_send.at[0])
        all_sent(rows_out.at[:, 0], out_send.at[0])

    sums = [
        pltpu.make_async_copy(up_sum_ref, up_total, sum_sem.at[UP]),
        pltpu.make_async_copy(down_sum_ref, down_total, sum_sem.at[DOWN]),
    ]
    for one in keep + sums:
        one.start()
    ends = (back_end, mixed_end)
    jobs = {
        TOK: send_tok, PAIR: pair_begin, LINE: line_begin, LINE_PASS: line_pass, CORE: to_core,
        PRE: saved_pre, GRAD: saved_grad, SHARE: grad_share, KEEP: grad_keep, GRAD_LINE: grad_begin, GRAD_GO: grad_go,
        GRAD_PAIR: grad_spread, GRAD_REP: grad_pass, BACK_SUMS: back_sums, MIXED_SUMS: mixed_sums,
        FIRST: part_first, SECOND: part_second, THIRD: part_third, LAST: lambda array: ends[array](),
        END: finish,
    }
    for job, *details in SCHEDULE:
        jobs[job](*details)


def store_kernel(*refs):
    count = len(refs) // 2
    copies = [
        pltpu.make_async_copy(refs[index], refs[count + index], refs[-1].at[index])
        for index in range(count)
    ]
    for one in copies:
        one.start()
    for one in copies:
        one.wait()


def cube_body(
    x_later, kept_input_rows, cotangent, norm_gain_vector, up_weight, down_weight, up_sum, down_sum
):
    row_count, width = x_later.shape
    n_fs = lax.axis_size("fs")
    grad_scale = float(row_count * lax.axis_size("rep") * n_fs) ** (-0.5)
    depth, units = up_weight.shape
    own = units // n_fs
    rows = row_count // 2
    outer = n_fs // 2
    tokens = n_fs * rows
    kind = x_later.dtype
    dma = pltpu.SemaphoreType.DMA
    vmem = functools.partial(pltpu.VMEM, dtype=kind)
    outside = pl.BlockSpec(memory_space=pltpu.HBM)
    results = pl.pallas_call(
        functools.partial(layer_kernel, n_fs, grad_scale),
        out_shape=(
            jax.ShapeDtypeStruct((2, 2, rows // 2, width), kind),
            jax.ShapeDtypeStruct((2, 2, rows // 2, width), kind),
            jax.ShapeDtypeStruct((depth, units), jnp.float32),
            jax.ShapeDtypeStruct((units, depth), jnp.float32),
        ),
        in_specs=[outside] * 8,
        out_specs=[pl.BlockSpec(memory_space=pl.ANY)] * 4,
        scratch_shapes=[
            pltpu.VMEM((1, width), jnp.float32), vmem((rows, width)), vmem((rows, width)), vmem((3, n_fs, 2, rows // 2, width)),
            vmem((2, width, own)), vmem((2, own, width)), vmem((depth, own)), vmem((own, depth)),
            pltpu.VMEM((2, tokens, own), jnp.float32), vmem((2, n_fs, 2, rows // 2, own)), vmem((2, n_fs, 2, rows // 2, own)),
            pltpu.VMEM((2, own, width), jnp.float32),
            vmem((2, own, width)), vmem((2, own, width)), vmem((2, own, width)),
            vmem((3, 2, 2, own, depth)), vmem((2, 2, own, depth)), vmem((2, n_fs, own, depth)),
            vmem((2, n_fs, 2, rows // 2, width)),
            vmem((2, 2, 4, rows // 2, width)), vmem((2, 2, 2, rows // 2, width)),
            vmem((2, 2, rows // 2, width)), vmem((2, 2, 2, rows // 2, width)),
            pltpu.VMEM((depth, units), jnp.float32), pltpu.VMEM((units, depth), jnp.float32),
            dma((5,)), dma((1,)), dma((2,)), dma((1,)), dma((3, 2)), dma((1,)), dma((2,)), dma((2,)),
            dma((1,)), dma((3, 2, 3)), dma((3, 2)), dma((1,)), dma((2,)), dma((1,)), dma((2, 2)),
            dma((1,)), dma((2,)), dma((1,)), dma((2, 2)), dma((1,)), dma((2, 2, 3)), dma((2,)),
            dma((1,)), dma((2,)), dma((2,)), dma((3,)),
        ],
        compiler_params=pltpu.CompilerParams(
            collective_id=0, has_side_effects=True, vmem_limit_bytes=VMEM_BYTES
        ),
    )(
        *[
            pltpu.with_memory_space_constraint(values, pltpu.HBM)
            for values in (
                x_later, kept_input_rows, cotangent, norm_gain_vector.reshape(1, width),
                up_weight, down_weight, up_sum, down_sum,
            )
        ],
    )
    results = [one.reshape(row_count, width) for one in results[:2]] + list(results[2:])
    return pl.pallas_call(
        store_kernel,
        out_shape=[jax.ShapeDtypeStruct(one.shape, one.dtype) for one in results],
        in_specs=[pl.BlockSpec(memory_space=pl.ANY)] * len(results),
        out_specs=[pl.BlockSpec(memory_space=pl.ANY)] * len(results),
        scratch_shapes=[dma((len(results),))],
        compiler_params=pltpu.CompilerParams(vmem_limit_bytes=2**20),
    )(*results)


def chosen_body(*args):
    depth, units = args[4].shape
    n_fs = lax.axis_size("fs")
    cubes = lax.axis_size("tp") == 2 and lax.axis_size("rep") == 2 and n_fs == 8
    return (cube_body if cubes and units == depth * n_fs and depth % 128 == 0 else body)(*args)


def solution(mesh):
    return jax.shard_map(
        chosen_body,
        mesh=mesh,
        in_specs=(
            P(("rep", "fs"), None),
            P(("rep", "fs"), None),
            P(("rep", "fs"), None),
            P(),
            P("fs", "tp"),
            P("tp", "fs"),
            P("fs", "tp"),
            P("tp", "fs"),
        ),
        out_specs=(P(("rep", "fs"), None), P(("rep", "fs"), None), P("fs", "tp"), P("tp", "fs")),
        check_vma=False,
    )
```
